32 devices in a mesh: dp: 4 (over y, x), kv: 4 (over z), tp: 2 (over core).
Axes of the slice: x: 2, y: 2, z: 4, core: 2. Of those that a mesh axis runs over, the one named last changes fastest.
Arguments:
- tokens: bfloat16 [32, 2048], P('dp', ('kv', 'tp')), parts along dimension 0, may hold values from -8 to 8
- mlp1_gain: float32 [2048], replicated, may hold values from 0.1 to 1.9
- mlp1_gate: bfloat16 [2048, 5632], P(None, ('kv', 'tp')), may hold values from -0.125 to 0.125
- mlp1_up: bfloat16 [2048, 5632], P(None, ('kv', 'tp')), may hold values from -0.125 to 0.125
- mlp1_down: bfloat16 [5632, 2048], P(('kv', 'tp')), may hold values from -0.109375 to 0.109375
- mixer_gain: float32 [2048], replicated, may hold values from 0.1 to 1.9
- proj_z: bfloat16 [2048, 2048], P('kv', 'tp'), may hold values from -0.125 to 0.125
- proj_x: bfloat16 [2048, 2048], P('kv', 'tp'), may hold values from -0.125 to 0.125
- proj_bc: bfloat16 [2048, 2, 512], P('kv', None, 'tp'), may hold values from -0.125 to 0.125
- proj_dt: bfloat16 [2048, 32], P('kv', 'tp'), may hold values from -0.125 to 0.125
- conv_x: bfloat16 [4, 2048], P(None, 'tp'), may hold values from -3 to 3
- conv_bc: bfloat16 [4, 2, 512], P(None, None, 'tp'), may hold values from -3 to 3
- window_x: bfloat16 [32, 3, 2048], P(('dp', 'kv'), None, 'tp'), parts along dimension 0, may hold values from -6 to 6
- window_bc: bfloat16 [32, 3, 2, 512], P(('dp', 'kv'), None, None, 'tp'), parts along dimension 0, may hold values from -6 to 6
- ssm_state: float32 [32, 32, 64, 128], P(('dp', 'kv'), 'tp'), parts along dimension 0, may hold values from -0.8 to 0.8
- dt_bias: float32 [32], P('tp'), may hold values from -4 to 0
- log_rate: float32 [32], P('tp'), may hold values from 0 to 2.77
- skip_gain: float32 [32], P('tp'), may hold values from 0.25 to 2
- group_gain: float32 [2048], P('tp'), may hold values from 0.1 to 1.9
- out_weight: bfloat16 [2048, 2048], P('tp', 'kv'), may hold values from -0.125 to 0.125
- mlp2_gain: float32 [2048], replicated, may hold values from 0.1 to 1.9
- mlp2_gate: bfloat16 [2048, 5632], P(None, ('kv', 'tp')), may hold values from -0.125 to 0.125
- mlp2_up: bfloat16 [2048, 5632], P(None, ('kv', 'tp')), may hold values from -0.125 to 0.125
- mlp2_down: bfloat16 [5632, 2048], P(('kv', 'tp')), may hold values from -0.109375 to 0.109375
Outputs:
- result: bfloat16 [32, 2048], P('dp', ('kv', 'tp')), parts along dimension 0
- new_state: float32 [32, 32, 64, 128], P(('dp', 'kv'), 'tp'), parts along dimension 0
- new_window_x: bfloat16 [32, 3, 2048], P(('dp', 'kv'), None, 'tp'), parts along dimension 0
- new_window_bc: bfloat16 [32, 3, 2, 512], P(('dp', 'kv'), None, None, 'tp'), parts along dimension 0
The draws below stay inside these ranges and needn't reach their ends.
There are 4 independent parts, one for each index of `dp`. The reference program is written for one: setup_inputs(seed, part) draws one part's arguments, and reference() takes and returns one part's arrays. A program takes and returns all parts, laid end to end along the dimension named above; an argument that names none is the same for every part. Nothing has to cross between parts.
All inputs are finite; a program needn't handle non-finite values.
Results may differ from the reference program's by a relative error of at most 0.013.
Values may be sent and summed in bfloat16 or wider, within the bound.
A program may use at most 64 MiB of HBM per device.

```python
import math
import jax
import jax.numpy as jnp
from jax import lax

D = 2048
FF = 5632
HEADS = 32
HEAD_DIM = 64
STATE = 128
GROUPS = 4
CONV_W = 4
BATCH = 8
N_TP = 2


def draw_tokens(key, part):
    position = jnp.arange(D, dtype=jnp.float32) / D
    column_scale = jnp.exp(math.log(6.0) * (position - 0.5))
    values = jax.random.normal(jax.random.fold_in(key, 11), (BATCH, D), jnp.float32) * column_scale
    return jnp.clip(values, -8.0, 8.0).astype(jnp.bfloat16)


def strengthened(values, rng, source, target, shards_of, factor):
    owner, partner = [(jnp.arange(values.shape[axis_at]) // (values.shape[axis_at] // shards_of)).reshape([-1 if axis == axis_at else 1 for axis in range(values.ndim)]) for axis_at in (source, target)]
    chosen = jax.random.permutation(rng, shards_of)[partner]
    strong = (owner == chosen) | (owner == (partner + shards_of // 2) % shards_of)
    return jnp.where(strong, factor * values, values)


def steps_of(stream_key, extent, pieces, smallest, high):
    gain, own = 1.0, jax.random.fold_in(stream_key, 6)
    for dim, blocks in pieces:
        steps = jnp.exp(jax.random.uniform(jax.random.fold_in(own, dim), (blocks,), jnp.float32, smallest / len(pieces), high / len(pieces)))
        gain = gain * jnp.repeat(steps, extent[dim] // blocks).reshape([-1 if axis == dim else 1 for axis in range(len(extent))])
    return gain


def noise(rng, shape, width, reach, cuts=(), held_as=jnp.bfloat16):
    level = steps_of(rng, shape, cuts, -0.22, 0.18) if cuts else 1.0
    values = jax.random.normal(rng, shape, jnp.float32) * width * level
    return jnp.minimum(jnp.maximum(values, -reach), reach).astype(held_as)


def gaussian_with(rng, dims, scale, reach, pieces, heavy, kind=jnp.bfloat16):
    values = scale * jax.random.normal(rng, dims, jnp.float32)
    if pieces:
        values = values * steps_of(rng, dims, pieces, -0.22, 0.18)
    return jnp.clip(strengthened(values, jax.random.fold_in(rng, 3), *heavy), -reach, reach).astype(kind)


def setup_inputs(seed: int = 0, part: int = 0) -> dict:
    key_list = jax.random.split(jax.random.key(seed), 25)
    part_splits = jax.random.split(jax.random.fold_in(key_list[24], part), 25)
    return {
        "tokens": draw_tokens(jax.random.fold_in(jax.random.fold_in(key_list[24], part), 71), part),
        "mlp1_gain": jnp.clip(1.0 + 0.18 * jax.random.normal(key_list[1], (D,), jnp.float32), 0.1, 1.9),
        "mlp1_gate": noise(key_list[2], (D, FF), D ** -0.5, 0.125, ((1, 8),)),
        "mlp1_up": noise(key_list[3], (D, FF), D ** -0.5, 0.125, ((1, 8),)),
        "mlp1_down": gaussian_with(key_list[4], (FF, D), FF ** -0.5, 0.109375, ((0, 8),), (0, 1, 8, 2.0)),
        "mixer_gain": jnp.clip(1.0 + 0.18 * jax.random.normal(key_list[5], (D,), jnp.float32), 0.1, 1.9),
        "proj_z": noise(key_list[6], (D, HEADS * HEAD_DIM), D ** -0.5, 0.125, ((0, 4), (1, 2))),
        "proj_x": noise(key_list[7], (D, HEADS * HEAD_DIM), D ** -0.5, 0.125, ((0, 4), (1, 2))),
        "proj_bc": noise(key_list[8], (D, 2, GROUPS * STATE), D ** -0.5, 0.125, ((0, 4), (2, 2))),
        "proj_dt": noise(key_list[9], (D, HEADS), D ** -0.5, 0.125, ((0, 4), (1, 2))),
        "conv_x": noise(key_list[10], (CONV_W, HEADS * HEAD_DIM), CONV_W ** -0.5, 3.0, ((1, 2),)),
        "conv_bc": noise(key_list[11], (CONV_W, 2, GROUPS * STATE), CONV_W ** -0.5, 3.0, ((2, 2),)),
        "window_x": noise(part_splits[12], (BATCH, CONV_W - 1, HEADS * HEAD_DIM), 1.0, 6.0, ((0, 4), (2, 2))),
        "window_bc": noise(part_splits[13], (BATCH, CONV_W - 1, 2, GROUPS * STATE), 1.0, 6.0, ((0, 4), (3, 2))),
        "ssm_state": noise(part_splits[14], (BATCH, HEADS, HEAD_DIM, STATE), 0.1, 0.8, ((0, 4), (1, 2)), jnp.float32),
        "dt_bias": jnp.clip(-4.0 + 4.0 * jax.random.uniform(key_list[15], (HEADS,), jnp.float32) ** steps_of(key_list[15], (HEADS,), ((0, 2),), -0.2, 0.2), -4.0, 0.0),
        "log_rate": jnp.clip(2.77 * jax.random.uniform(key_list[16], (HEADS,), jnp.float32) ** steps_of(key_list[16], (HEADS,), ((0, 2),), -0.2, 0.2), 0.0, 2.77),
        "skip_gain": jnp.clip(0.25 + 1.75 * jax.random.uniform(key_list[17], (HEADS,), jnp.float32) ** steps_of(key_list[17], (HEADS,), ((0, 2),), -0.2, 0.2), 0.25, 2.0),
        "group_gain": jnp.clip(1.0 + 0.18 * jax.random.normal(key_list[18], (HEADS * HEAD_DIM,), jnp.float32), 0.1, 1.9),
        "out_weight": noise(key_list[19], (HEADS * HEAD_DIM, D), (HEADS * HEAD_DIM) ** -0.5, 0.125, ((0, 2), (1, 4))),
        "mlp2_gain": jnp.clip(1.0 + 0.18 * jax.random.normal(key_list[20], (D,), jnp.float32), 0.1, 1.9),
        "mlp2_gate": noise(key_list[21], (D, FF), D ** -0.5, 0.125, ((1, 8),)),
        "mlp2_up": noise(key_list[22], (D, FF), D ** -0.5, 0.125, ((1, 8),)),
        "mlp2_down": gaussian_with(key_list[23], (FF, D), FF ** -0.5, 0.109375, ((0, 8),), (0, 1, 8, 2.0)),
    }


EPS = 1e-06

def norm_rows(values, scale_gain):
    floats = values.astype(jnp.float32)
    factor = jax.lax.rsqrt(lax.optimization_barrier(jnp.mean(floats * floats, axis=-1, keepdims=True)) + EPS)
    return (floats * factor * scale_gain.astype(jnp.float32)).astype(jnp.bfloat16)

def half_mlp(columns, scale_gain, gate_weight, up_weight, down_weight):
    normed = norm_rows(columns, scale_gain)
    gate_part = jnp.dot(normed, gate_weight, preferred_element_type=jnp.float32)
    up_part = jnp.dot(normed, up_weight, preferred_element_type=jnp.float32)
    hidden = (jax.nn.silu(gate_part) * up_part).astype(jnp.bfloat16)
    summed = jnp.dot(hidden, down_weight, preferred_element_type=jnp.float32)
    return (columns.astype(jnp.float32) + 0.5 * summed).astype(jnp.bfloat16)

def reference(tokens, mlp1_gain, mlp1_gate, mlp1_up, mlp1_down, mixer_gain, proj_z, proj_x, proj_bc, proj_dt, conv_x, conv_bc, window_x, window_bc, ssm_state, dt_bias, log_rate, skip_gain, group_gain, out_weight, mlp2_gain, mlp2_gate, mlp2_up, mlp2_down):
    after_first = half_mlp(tokens, mlp1_gain, mlp1_gate, mlp1_up, mlp1_down)
    normed = norm_rows(after_first, mixer_gain)
    inner_width = HEADS * HEAD_DIM
    group_width = GROUPS * STATE
    gate_z = jnp.dot(normed, proj_z, preferred_element_type=jnp.float32).astype(jnp.bfloat16)
    x_new = jnp.dot(normed, proj_x, preferred_element_type=jnp.float32).astype(jnp.bfloat16)
    bc_new = jnp.dot(normed, proj_bc.reshape(D, 2 * group_width), preferred_element_type=jnp.float32)
    bc_new = bc_new.astype(jnp.bfloat16).reshape(BATCH, 2, group_width)
    rate_raw = jnp.dot(normed, proj_dt, preferred_element_type=jnp.float32)
    full_x = jnp.concatenate([window_x, x_new[:, None]], axis=1)
    full_bc = jnp.concatenate([window_bc, bc_new[:, None]], axis=1)
    mixed_x = jax.nn.silu(jnp.einsum('sji,ji->si', full_x.astype(jnp.float32), conv_x.astype(jnp.float32)))
    mixed_bc = jax.nn.silu(jnp.einsum('sjci,jci->sci', full_bc.astype(jnp.float32), conv_bc.astype(jnp.float32)))
    repeat = HEADS // GROUPS
    inputs_x = mixed_x.reshape(BATCH, HEADS, HEAD_DIM)
    keys_b = jnp.repeat(mixed_bc[:, 0].reshape(BATCH, GROUPS, STATE), repeat, axis=1)
    reads_c = jnp.repeat(mixed_bc[:, 1].reshape(BATCH, GROUPS, STATE), repeat, axis=1)
    step_size = jax.nn.softplus(rate_raw + dt_bias)
    retain = jnp.exp(-step_size * jnp.exp(log_rate))
    new_state = retain[:, :, None, None] * ssm_state + (step_size[:, :, None] * inputs_x)[:, :, :, None] * keys_b[:, :, None, :]
    readout = jnp.einsum('shpn,shn->shp', new_state, reads_c) + skip_gain[None, :, None] * inputs_x
    gated = readout.reshape(BATCH, inner_width) * jax.nn.silu(gate_z.astype(jnp.float32))
    grouped = gated.reshape(BATCH, GROUPS, inner_width // GROUPS)
    grouped = grouped * jax.lax.rsqrt(lax.optimization_barrier(jnp.mean(grouped * grouped, axis=-1, keepdims=True)) + EPS)
    mixed = (grouped.reshape(BATCH, inner_width) * group_gain).astype(jnp.bfloat16)
    half_width = inner_width // N_TP
    summed_out = jnp.zeros((BATCH, D), jnp.float32)
    for section in range(N_TP):
        lower = section * half_width
        partial_out = jnp.dot(mixed[:, lower:lower + half_width], out_weight[lower:lower + half_width], preferred_element_type=jnp.float32)
        summed_out = summed_out + partial_out.astype(jnp.bfloat16).astype(jnp.float32)
    after_mixer = (after_first.astype(jnp.float32) + summed_out).astype(jnp.bfloat16)
    result = half_mlp(after_mixer, mlp2_gain, mlp2_gate, mlp2_up, mlp2_down)
    return (result, new_state, full_x[:, 1:], full_bc[:, 1:])
```

```python
import functools

import jax
import jax.numpy as jnp
from jax import lax
from jax.experimental import pallas as pl
from jax.experimental.pallas import tpu as pltpu
from jax.sharding import PartitionSpec as P

EPS = 1e-06


def norm_rows(values, scale_gain):
    floats = values.astype(jnp.float32)
    factor = lax.rsqrt(jnp.mean(floats * floats, axis=-1, keepdims=True) + EPS)
    return (floats * factor * scale_gain).astype(jnp.bfloat16)


def half_mlp(columns, scale_gain, gate_weight, up_weight, down_weight):
    gathered = lax.all_gather(columns, ("kv", "tp"), axis=1, tiled=True)
    normed = norm_rows(gathered, scale_gain)
    gate_part = jnp.dot(normed, gate_weight, preferred_element_type=jnp.float32)
    up_part = jnp.dot(normed, up_weight, preferred_element_type=jnp.float32)
    hidden = (jax.nn.silu(gate_part) * up_part).astype(jnp.bfloat16)
    partial_sums = jnp.dot(hidden, down_weight, preferred_element_type=jnp.float32)
    summed = lax.psum_scatter(partial_sums, ("kv", "tp"), scatter_dimension=1, tiled=True)
    return (columns.astype(jnp.float32) + 0.5 * summed).astype(jnp.bfloat16)


def plain_device(
    tokens,
    mlp1_gain,
    mlp1_gate,
    mlp1_up,
    mlp1_down,
    mixer_gain,
    proj_z,
    proj_x,
    proj_bc,
    proj_dt,
    conv_x,
    conv_bc,
    window_x,
    window_bc,
    ssm_state,
    dt_bias,
    log_rate,
    skip_gain,
    group_gain,
    out_weight,
    mlp2_gain,
    mlp2_gate,
    mlp2_up,
    mlp2_down,
):
    after_first = half_mlp(tokens, mlp1_gain, mlp1_gate, mlp1_up, mlp1_down)
    kv_width = proj_z.shape[0]
    kv_offset = lax.axis_index("kv") * kv_width
    gathered = lax.all_gather(after_first, ("kv", "tp"), axis=1, tiled=True)
    floats = gathered.astype(jnp.float32)
    squares = jnp.sum(floats * floats, axis=1)
    own_cols = lax.dynamic_slice_in_dim(gathered, kv_offset, kv_width, 1)
    model_width = kv_width * lax.axis_size("kv")
    factor = lax.rsqrt(squares / model_width + EPS)
    gain_cols = lax.dynamic_slice_in_dim(mixer_gain, kv_offset, kv_width, 0)
    normed = (own_cols.astype(jnp.float32) * factor[:, None] * gain_cols).astype(jnp.bfloat16)
    inner_width = proj_z.shape[1]
    group_width = proj_bc.shape[2]
    joined = jnp.concatenate(
        [proj_z, proj_x, proj_bc.reshape(kv_width, 2 * group_width), proj_dt], axis=1
    )
    own_seqs = window_x.shape[0]
    projected = lax.psum_scatter(
        jnp.dot(normed, joined, preferred_element_type=jnp.float32),
        "kv",
        scatter_dimension=0,
        tiled=True,
    )
    gate_z = projected[:, :inner_width].astype(jnp.bfloat16)
    x_new = projected[:, inner_width : 2 * inner_width].astype(jnp.bfloat16)
    bc_end = 2 * inner_width + 2 * group_width
    bc_new = (
        projected[:, 2 * inner_width : bc_end]
        .astype(jnp.bfloat16)
        .reshape(own_seqs, 2, group_width)
    )
    rate_raw = projected[:, bc_end:]
    full_x = jnp.concatenate([window_x, x_new[:, None]], axis=1)
    full_bc = jnp.concatenate([window_bc, bc_new[:, None]], axis=1)
    mixed_x = jax.nn.silu(
        jnp.einsum("sji,ji->si", full_x.astype(jnp.float32), conv_x.astype(jnp.float32))
    )
    mixed_bc = jax.nn.silu(
        jnp.einsum("sjci,jci->sci", full_bc.astype(jnp.float32), conv_bc.astype(jnp.float32))
    )
    heads = proj_dt.shape[1]
    state_size = ssm_state.shape[3]
    groups = group_width // state_size
    head_dim = inner_width // heads
    repeat = heads // groups
    inputs_x = mixed_x.reshape(own_seqs, heads, head_dim)
    keys_b = jnp.repeat(mixed_bc[:, 0].reshape(own_seqs, groups, state_size), repeat, axis=1)
    reads_c = jnp.repeat(mixed_bc[:, 1].reshape(own_seqs, groups, state_size), repeat, axis=1)
    step_size = jax.nn.softplus(rate_raw + dt_bias)
    retain = jnp.exp(-step_size * jnp.exp(log_rate))
    new_state = (
        retain[:, :, None, None] * ssm_state
        + (step_size[:, :, None] * inputs_x)[:, :, :, None] * keys_b[:, :, None, :]
    )
    readout = jnp.einsum("shpn,shn->shp", new_state, reads_c) + skip_gain[None, :, None] * inputs_x
    gated = readout.reshape(own_seqs, inner_width) * jax.nn.silu(gate_z.astype(jnp.float32))
    grouped = gated.reshape(own_seqs, groups, inner_width // groups)
    grouped = grouped * lax.rsqrt(jnp.mean(grouped * grouped, axis=-1, keepdims=True) + EPS)
    mixed = (grouped.reshape(own_seqs, inner_width) * group_gain).astype(jnp.bfloat16)
    partial_out = jnp.dot(
        lax.all_gather(mixed, "kv", axis=0, tiled=True),
        out_weight,
        preferred_element_type=jnp.float32,
    )
    summed_out = lax.psum_scatter(
        partial_out.astype(jnp.bfloat16), "tp", scatter_dimension=1, tiled=True
    ).astype(jnp.float32)
    after_mixer = (after_first.astype(jnp.float32) + summed_out).astype(jnp.bfloat16)
    result = half_mlp(after_mixer, mlp2_gain, mlp2_gate, mlp2_up, mlp2_down)
    return (result, new_state, full_x[:, 1:], full_bc[:, 1:])


MESH = pl.DeviceIdType.MESH
F32 = jnp.float32
BF16 = jnp.bfloat16
TOKENS, SUM1, PROJ, EXTRA, FIRST, MIXED, OUT, SUM2 = range(8)
PHASES = 8


def dot32(left, right):
    return jnp.dot(left, right, preferred_element_type=F32)


def fused_kernel(
    n_kv,
    n_tp,
    tokens,
    gain1,
    gate1,
    up1,
    down1,
    gain_m,
    proj_z,
    proj_x,
    proj_bc,
    proj_dt,
    conv_x,
    conv_bc,
    window_x,
    window_bc,
    state,
    dt_bias,
    log_rate,
    skip_gain,
    group_gain,
    out_weight,
    gain2,
    gate2,
    up2,
    down2,
    result,
    step_x_out,
    retain_out,
    b_out,
    x_new_out,
    bc_new_out,
    tok_v,
    gain1_v,
    gate1_v,
    up1_v,
    down1_v,
    gain_m_v,
    z_v,
    x_v,
    bc_v,
    dt_v,
    conv_x_v,
    conv_bc_v,
    window_x_v,
    window_bc_v,
    state_v,
    bias_v,
    log_v,
    skip_v,
    ggain_v,
    out_v,
    gain2_v,
    gate2_v,
    up2_v,
    down2_v,
    state_half,
    tok_all,
    sum1_send,
    sum1_all,
    proj_send,
    proj_all,
    extra_send,
    extra_all,
    first_all,
    mixed_all,
    out_all,
    sum2_send,
    sum2_all,
    local_sem,
    send_sem,
    recv_sem,
):
    n = n_kv * n_tp
    kv, tp = lax.axis_index("kv"), lax.axis_index("tp")
    me = kv * n_tp + tp
    rows, cols = tok_v.shape
    width = cols * n
    kv_cols = cols * n_tp
    used = [0]

    def load(source, target):
        copy = pltpu.make_async_copy(source, target, local_sem.at[used[0]])
        used[0] += 1
        copy.start()
        return copy

    chunk = cols
    tok_copies = [load(tokens, tok_v), load(gain1, gain1_v)]
    gu1 = []
    for i in range(n):
        part = pl.ds(i * chunk, chunk)
        gu1.append((load(gate1.at[part], gate1_v.at[part]), load(up1.at[part], up1_v.at[part])))
    down1_copy = load(down1, down1_v)
    proj_copies = [
        load(gain_m, gain_m_v),
        load(proj_z, z_v),
        load(proj_x, x_v),
        load(proj_bc, bc_v),
        load(proj_dt, dt_v),
    ]
    ssm_copies = [
        load(conv_x, conv_x_v),
        load(conv_bc, conv_bc_v),
        load(window_x, window_x_v),
        load(window_bc, window_bc_v),
        load(dt_bias, bias_v),
        load(log_rate, log_v),
        load(skip_gain, skip_v),
        load(group_gain, ggain_v),
        load(state, state_v),
    ]
    out_copy = load(out_weight, out_v)
    gain2_copy = load(gain2, gain2_v)
    gu2 = [load(gate2, gate2_v), load(up2, up2_v)]
    down2_copy = load(down2, down2_v)

    def peer_of(offset):
        peer = lax.rem(me + offset, n)
        return peer, lax.div(peer, n_tp), lax.rem(peer, n_tp)

    barrier = pltpu.get_barrier_semaphore()
    for offset in range(1, n):
        _, peer_kv, peer_tp = peer_of(offset)
        pl.semaphore_signal(
            barrier, inc=1, device_id={"kv": peer_kv, "tp": peer_tp}, device_id_type=MESH
        )
    pl.semaphore_wait(barrier, n - 1)

    sends = []

    def send(source, target, phase, slot, source_slot, to_kv, to_tp):
        copy = pltpu.make_async_remote_copy(
            src_ref=source,
            dst_ref=target,
            send_sem=send_sem.at[phase, slot],
            recv_sem=recv_sem.at[phase, source_slot],
            device_id={"kv": to_kv, "tp": to_tp},
            device_id_type=MESH,
        )
        copy.start()
        sends.append(copy)

    def arrive(target, phase, source_slot):
        pltpu.make_async_remote_copy(
            src_ref=target,
            dst_ref=target,
            send_sem=send_sem.at[phase, 0],
            recv_sem=recv_sem.at[phase, source_slot],
            device_id={"kv": kv, "tp": tp},
            device_id_type=MESH,
        ).wait_recv()

    for copy in tok_copies:
        copy.wait()
    for offset in range(1, n):
        _, peer_kv, peer_tp = peer_of(offset)
        send(tok_v, tok_all.at[me], TOKENS, offset, me, peer_kv, peer_tp)
    tok_all[me] = tok_v[...]
    for offset in range(1, n):
        peer, _, _ = peer_of(offset)
        arrive(tok_all.at[peer], TOKENS, peer)

    def hidden_of(parts, gain_ref, gate_ref, up_ref, ready):
        squares = sum(jnp.sum(v * v, axis=1, keepdims=True) for v in parts)
        factor = lax.rsqrt(squares / width + EPS)
        gate_part = up_part = None
        for i, v in enumerate(parts):
            piece = v.shape[1]
            part = pl.ds(i * piece, piece)
            normed = (v * factor * gain_ref[:, part]).astype(BF16)
            ready(i)
            a, b = dot32(normed, gate_ref[part, :]), dot32(normed, up_ref[part, :])
            gate_part = a if i == 0 else gate_part + a
            up_part = b if i == 0 else up_part + b
        return (jax.nn.silu(gate_part) * up_part).astype(BF16)

    def ready1(i):
        for copy in gu1[i]:
            copy.wait()

    hidden1 = hidden_of(
        [tok_all[i].astype(F32) for i in range(n)], gain1_v, gate1_v, up1_v, ready1
    )
    down1_copy.wait()
    for step in range(1, n_kv + 1):
        to_kv = lax.rem(kv + step, n_kv)
        part = pl.ds(pl.multiple_of(to_kv * kv_cols, 128), kv_cols)
        partial_sum = dot32(hidden1, down1_v[:, part]).astype(BF16)
        if step < n_kv:
            sum1_send[step] = partial_sum
            for other in range(n_tp):
                to_tp = lax.rem(tp + other, n_tp)
                send(
                    sum1_send.at[step],
                    sum1_all.at[me],
                    SUM1,
                    step * n_tp + other,
                    me,
                    to_kv,
                    to_tp,
                )
        else:
            sum1_all[me] = partial_sum
            sum1_send[0] = partial_sum
            for other in range(1, n_tp):
                to_tp = lax.rem(tp + other, n_tp)
                send(sum1_send.at[0], sum1_all.at[me], SUM1, other, me, kv, to_tp)

    for copy in ssm_copies:
        copy.wait()
    seqs = window_x_v.shape[0]
    state_size = state_v.shape[2]
    heads = dt_v.shape[1]
    inner = z_v.shape[1]
    group_width = bc_v.shape[1] // 2
    groups = group_width // state_size
    head_dim = inner // heads
    group_inner = inner // groups
    taps = conv_x_v.shape[0]
    conv_xf = conv_x_v[...].astype(F32)
    past_x = jnp.concatenate(
        [
            jnp.sum(window_x_v[s].astype(F32) * conv_xf[: taps - 1], axis=0, keepdims=True)
            for s in range(seqs)
        ],
        axis=0,
    )
    conv_bcf = conv_bc_v[...].astype(F32)
    past_bc = jnp.concatenate(
        [
            jnp.sum(window_bc_v[s].astype(F32) * conv_bcf[: taps - 1], axis=0, keepdims=True)
            for s in range(seqs)
        ],
        axis=0,
    )
    state_half[...] = state_v[...].astype(BF16)
    lanes = lax.broadcasted_iota(jnp.int32, (heads, inner), 1)
    owner = lax.broadcasted_iota(jnp.int32, (heads, inner), 0)
    low = owner * head_dim
    spread = jnp.where((lanes >= low) & (lanes < low + head_dim), 1.0, 0.0).astype(F32)

    def expand(values):
        return jnp.dot(
            values, spread, preferred_element_type=F32, precision=lax.Precision.HIGHEST
        )

    skip = expand(jnp.broadcast_to(skip_v[...], (8, heads)))[:seqs]
    for copy in proj_copies:
        copy.wait()

    for offset in range(1, n):
        peer, _, _ = peer_of(offset)
        arrive(sum1_all.at[peer], SUM1, peer)
    summed = sum1_all[0].astype(F32)
    for i in range(1, n):
        summed = summed + sum1_all[i].astype(F32)
    base = jnp.concatenate([tok_all[kv * n_tp + t].astype(F32) for t in range(n_tp)], axis=1)
    after = (base + 0.5 * summed).astype(BF16)
    first_all[kv] = after
    after32 = after.astype(F32)
    squares = jnp.sum(after32 * after32, axis=1, keepdims=True)
    gain_part = gain_m_v[:, pl.ds(pl.multiple_of(kv * kv_cols, 128), kv_cols)]
    scaled = (after32 * gain_part).astype(BF16)
    own_rates = dot32(scaled, dt_v[...])
    for k in range(n_kv):
        rows_k = slice(k * seqs, (k + 1) * seqs)
        extra_send[k] = jnp.broadcast_to(squares[rows_k], (seqs, extra_send.shape[2]))
        extra_send[k, :, :heads] = own_rates[rows_k]
    for place, weight in ((0, z_v), (inner, x_v), (2 * inner, bc_v)):
        piece = dot32(scaled, weight[...])
        for k in range(n_kv):
            proj_send[k, :, pl.ds(place, weight.shape[1])] = piece[
                k * seqs : (k + 1) * seqs
            ].astype(BF16)
    proj_all[kv] = proj_send[kv]
    extra_all[kv] = extra_send[kv]
    for step in range(1, n_kv):
        to_kv = lax.rem(kv + step, n_kv)
        send(proj_send.at[to_kv], proj_all.at[kv], PROJ, step, kv, to_kv, tp)
        send(extra_send.at[to_kv], extra_all.at[kv], EXTRA, step, kv, to_kv, tp)
    for step in range(1, n_kv):
        to_kv = lax.rem(kv + step, n_kv)
        send(first_all.at[kv], first_all.at[kv], FIRST, step, kv, to_kv, tp)

    for step in range(1, n_kv):
        from_kv = lax.rem(kv + step, n_kv)
        arrive(extra_all.at[from_kv], EXTRA, from_kv)
        arrive(proj_all.at[from_kv], PROJ, from_kv)
    extra = extra_all[0]
    projected = proj_all[0].astype(F32)
    for k in range(1, n_kv):
        extra = extra + extra_all[k]
        projected = projected + proj_all[k].astype(F32)
    factor = lax.rsqrt(extra[:, heads : heads + 1] / width + EPS)
    projected = projected * factor
    step_size = extra[:, :heads] * factor + bias_v[...]
    step_size = jnp.maximum(step_size, 0.0) + jnp.log1p(jnp.exp(-jnp.abs(step_size)))
    retain = jnp.exp(-step_size * jnp.exp(log_v[...]))
    gate_z = projected[:, :inner].astype(BF16).astype(F32)
    x_new = projected[:, inner : 2 * inner].astype(BF16)
    bc_new = projected[:, 2 * inner :].astype(BF16)
    mixed_x = jax.nn.silu(past_x + conv_xf[taps - 1 :] * x_new.astype(F32))
    mixed_bc = jax.nn.silu(past_bc + conv_bcf[taps - 1 :] * bc_new.astype(F32))
    step_x = expand(step_size) * mixed_x
    retained = expand(retain)
    pieces = []
    which = lax.broadcasted_iota(jnp.int32, (seqs, group_inner), 0)
    for g in range(groups):
        b = mixed_bc[:, g * state_size : (g + 1) * state_size]
        c = mixed_bc[:, group_width + g * state_size : group_width + (g + 1) * state_size]
        span = slice(g * group_inner, (g + 1) * group_inner)
        old = None
        for s in range(seqs):
            read = lax.dot_general(
                c.astype(BF16),
                state_half[s, g * group_inner : (g + 1) * group_inner, :],
                (((1,), (1,)), ((), ())),
                preferred_element_type=F32,
            )
            old = read if s == 0 else jnp.where(which == s, read, old)
        match = jnp.sum(b * c, axis=1, keepdims=True)
        readout = retained[:, span] * old + step_x[:, span] * match + skip[:, span] * mixed_x[:, span]
        z = gate_z[:, span]
        gated = readout * jax.nn.silu(z)
        gated = gated * lax.rsqrt(jnp.mean(gated * gated, axis=1, keepdims=True) + EPS)
        pieces.append((gated * ggain_v[:, span]).astype(BF16))
    mixed_all[kv] = jnp.concatenate(pieces, axis=1)
    for step in range(1, n_kv):
        to_kv = lax.rem(kv + step, n_kv)
        send(mixed_all.at[kv], mixed_all.at[kv], MIXED, step, kv, to_kv, tp)
    step_x_out[...] = step_x
    retain_out[...] = retain
    b_out[...] = mixed_bc[:, :group_width]
    x_new_out[...] = x_new
    bc_new_out[...] = bc_new
    out_copy.wait()
    for step in range(1, n_kv):
        from_kv = lax.rem(kv + step, n_kv)
        arrive(mixed_all.at[from_kv], MIXED, from_kv)
    mixed = jnp.concatenate([mixed_all[k].astype(F32) for k in range(n_kv)], axis=0)
    out_all[me] = dot32(mixed.astype(BF16), out_v[...]).astype(BF16)
    for offset in range(1, n):
        _, peer_kv, peer_tp = peer_of(offset)
        send(out_all.at[me], out_all.at[me], OUT, offset, me, peer_kv, peer_tp)

    gain2_copy.wait()
    for copy in gu2:
        copy.wait()
    down2_copy.wait()
    for step in range(1, n_kv):
        from_kv = lax.rem(kv + step, n_kv)
        arrive(first_all.at[from_kv], FIRST, from_kv)
    for offset in range(1, n):
        peer, _, _ = peer_of(offset)
        arrive(out_all.at[peer], OUT, peer)

    def after_of(k):
        total = out_all[k * n_tp].astype(F32)
        for t in range(1, n_tp):
            total = total + out_all[k * n_tp + t].astype(F32)
        return (first_all[k].astype(F32) + total).astype(BF16).astype(F32)

    hidden2 = hidden_of(
        [after_of(k) for k in range(n_kv)], gain2_v, gate2_v, up2_v, lambda i: None
    )
    for offset in range(1, n + 1):
        peer, peer_kv, peer_tp = peer_of(offset)
        part = pl.ds(pl.multiple_of(peer * cols, 128), cols)
        partial_sum = dot32(hidden2, down2_v[:, part]).astype(BF16)
        if offset < n:
            sum2_send[offset] = partial_sum
            send(sum2_send.at[offset], sum2_all.at[me], SUM2, offset, me, peer_kv, peer_tp)
        else:
            sum2_all[me] = partial_sum
    own = after_of(kv)
    mine = own[:, :cols]
    for t in range(1, n_tp):
        mine = jnp.where(tp == t, own[:, t * cols : (t + 1) * cols], mine)
    for offset in range(1, n):
        peer, _, _ = peer_of(offset)
        arrive(sum2_all.at[peer], SUM2, peer)
    summed = sum2_all[0].astype(F32)
    for i in range(1, n):
        summed = summed + sum2_all[i].astype(F32)
    result[...] = (mine + 0.5 * summed).astype(BF16)
    for copy in sends:
        copy.wait_send()


def per_device(n_kv, n_tp, *args):
    (
        tokens,
        mlp1_gain,
        mlp1_gate,
        mlp1_up,
        mlp1_down,
        mixer_gain,
        proj_z,
        proj_x,
        proj_bc,
        proj_dt,
        conv_x,
        conv_bc,
        window_x,
        window_bc,
        ssm_state,
        dt_bias,
        log_rate,
        skip_gain,
        group_gain,
        out_weight,
        mlp2_gain,
        mlp2_gate,
        mlp2_up,
        mlp2_down,
    ) = args
    rows, cols = tokens.shape
    if cols % 128 or n_kv * n_tp > 16 or rows % 8:
        return plain_device(*args)
    n = n_kv * n_tp
    kv_cols = cols * n_tp
    seqs, heads = window_x.shape[0], proj_dt.shape[1]
    inner, group_width = proj_z.shape[1], proj_bc.shape[2]
    state_size = ssm_state.shape[3]
    groups = group_width // state_size
    taps = conv_x.shape[0]
    operands = (
        tokens,
        mlp1_gain[None],
        mlp1_gate,
        mlp1_up,
        mlp1_down,
        mixer_gain[None],
        proj_z,
        proj_x,
        proj_bc.reshape(proj_bc.shape[0], 2 * group_width),
        proj_dt,
        conv_x,
        conv_bc.reshape(taps, 2 * group_width),
        window_x,
        window_bc.reshape(seqs, taps - 1, 2 * group_width),
        ssm_state.reshape(seqs, inner, state_size),
        dt_bias[None],
        log_rate[None],
        skip_gain[None],
        group_gain[None],
        out_weight,
        mlp2_gain[None],
        mlp2_gate,
        mlp2_up,
        mlp2_down,
    )
    vmem = [pltpu.VMEM(a.shape, a.dtype) for a in operands]
    scratch = vmem + [
        pltpu.VMEM((seqs, inner, state_size), BF16),
        pltpu.VMEM((n, rows, cols), BF16),
        pltpu.VMEM((n_kv, rows, kv_cols), BF16),
        pltpu.VMEM((n, rows, kv_cols), BF16),
        pltpu.VMEM((n_kv, seqs, 2 * inner + 2 * group_width), BF16),
        pltpu.VMEM((n_kv, seqs, 2 * inner + 2 * group_width), BF16),
        pltpu.VMEM((n_kv, seqs, 128), F32),
        pltpu.VMEM((n_kv, seqs, 128), F32),
        pltpu.VMEM((n_kv, rows, kv_cols), BF16),
        pltpu.VMEM((n_kv, seqs, inner), BF16),
        pltpu.VMEM((n, rows, kv_cols), BF16),
        pltpu.VMEM((n, rows, cols), BF16),
        pltpu.VMEM((n, rows, cols), BF16),
        pltpu.SemaphoreType.DMA((2 * n + 40,)),
        pltpu.SemaphoreType.DMA((PHASES, n)),
        pltpu.SemaphoreType.DMA((PHASES, n)),
    ]
    shapes = (
        jax.ShapeDtypeStruct((rows, cols), BF16),
        jax.ShapeDtypeStruct((seqs, inner), F32),
        jax.ShapeDtypeStruct((seqs, heads), F32),
        jax.ShapeDtypeStruct((seqs, group_width), F32),
        jax.ShapeDtypeStruct((seqs, inner), BF16),
        jax.ShapeDtypeStruct((seqs, 2 * group_width), BF16),
    )
    result, step_x, retain, keys_b, x_new, bc_new = pl.pallas_call(
        functools.partial(fused_kernel, n_kv, n_tp),
        out_shape=shapes,
        in_specs=[pl.BlockSpec(memory_space=pl.ANY)] * len(operands),
        out_specs=[pl.BlockSpec(memory_space=pltpu.VMEM)] * len(shapes),
        scratch_shapes=scratch,
        compiler_params=pltpu.CompilerParams(
            collective_id=0, has_side_effects=True, vmem_limit_bytes=60 * 1024 * 1024
        ),
    )(*operands)
    keys_b = jnp.repeat(keys_b.reshape(seqs, groups, state_size), heads // groups, axis=1)
    new_state = (
        retain[:, :, None, None] * ssm_state
        + step_x.reshape(seqs, heads, inner // heads)[:, :, :, None] * keys_b[:, :, None, :]
    )
    new_x = jnp.concatenate([window_x[:, 1:], x_new[:, None]], axis=1)
    new_bc = jnp.concatenate(
        [window_bc[:, 1:], bc_new.reshape(seqs, 1, 2, group_width)], axis=1
    )
    return (result, new_state, new_x, new_bc)


def solution(mesh):
    placed = (
        P("dp", ("kv", "tp")),
        P(),
        P(None, ("kv", "tp")),
        P(None, ("kv", "tp")),
        P(("kv", "tp"), None),
        P(),
        P("kv", "tp"),
        P("kv", "tp"),
        P("kv", None, "tp"),
        P("kv", "tp"),
        P(None, "tp"),
        P(None, None, "tp"),
        P(("dp", "kv"), None, "tp"),
        P(("dp", "kv"), None, None, "tp"),
        P(("dp", "kv"), "tp", None, None),
        P("tp"),
        P("tp"),
        P("tp"),
        P("tp"),
        P("tp", "kv"),
        P(),
        P(None, ("kv", "tp")),
        P(None, ("kv", "tp")),
        P(("kv", "tp"), None),
    )
    return jax.shard_map(
        functools.partial(per_device, mesh.shape["kv"], mesh.shape["tp"]),
        mesh=mesh,
        in_specs=placed,
        out_specs=(
            P("dp", ("kv", "tp")),
            P(("dp", "kv"), "tp", None, None),
            P(("dp", "kv"), None, "tp"),
            P(("dp", "kv"), None, None, "tp"),
        ),
        check_vma=False,
    )
```

```python
import functools

import jax
import jax.numpy as jnp
from jax import lax
from jax.experimental import pallas as pl
from jax.experimental.pallas import tpu as pltpu
from jax.sharding import PartitionSpec as P

EPS = 1e-06


def norm_rows(values, scale_gain):
    floats = values.astype(jnp.float32)
    factor = lax.rsqrt(jnp.mean(floats * floats, axis=-1, keepdims=True) + EPS)
    return (floats * factor * scale_gain).astype(jnp.bfloat16)


def half_mlp(columns, scale_gain, gate_weight, up_weight, down_weight):
    gathered = lax.all_gather(columns, ("kv", "tp"), axis=1, tiled=True)
    normed = norm_rows(gathered, scale_gain)
    gate_part = jnp.dot(normed, gate_weight, preferred_element_type=jnp.float32)
    up_part = jnp.dot(normed, up_weight, preferred_element_type=jnp.float32)
    hidden = (jax.nn.silu(gate_part) * up_part).astype(jnp.bfloat16)
    partial_sums = jnp.dot(hidden, down_weight, preferred_element_type=jnp.float32)
    summed = lax.psum_scatter(partial_sums, ("kv", "tp"), scatter_dimension=1, tiled=True)
    return (columns.astype(jnp.float32) + 0.5 * summed).astype(jnp.bfloat16)


def plain_device(
    tokens,
    mlp1_gain,
    mlp1_gate,
    mlp1_up,
    mlp1_down,
    mixer_gain,
    proj_z,
    proj_x,
    proj_bc,
    proj_dt,
    conv_x,
    conv_bc,
    window_x,
    window_bc,
    ssm_state,
    dt_bias,
    log_rate,
    skip_gain,
    group_gain,
    out_weight,
    mlp2_gain,
    mlp2_gate,
    mlp2_up,
    mlp2_down,
):
    after_first = half_mlp(tokens, mlp1_gain, mlp1_gate, mlp1_up, mlp1_down)
    kv_width = proj_z.shape[0]
    kv_offset = lax.axis_index("kv") * kv_width
    gathered = lax.all_gather(after_first, ("kv", "tp"), axis=1, tiled=True)
    floats = gathered.astype(jnp.float32)
    squares = jnp.sum(floats * floats, axis=1)
    own_cols = lax.dynamic_slice_in_dim(gathered, kv_offset, kv_width, 1)
    model_width = kv_width * lax.axis_size("kv")
    factor = lax.rsqrt(squares / model_width + EPS)
    gain_cols = lax.dynamic_slice_in_dim(mixer_gain, kv_offset, kv_width, 0)
    normed = (own_cols.astype(jnp.float32) * factor[:, None] * gain_cols).astype(jnp.bfloat16)
    inner_width = proj_z.shape[1]
    group_width = proj_bc.shape[2]
    joined = jnp.concatenate(
        [proj_z, proj_x, proj_bc.reshape(kv_width, 2 * group_width), proj_dt], axis=1
    )
    own_seqs = window_x.shape[0]
    projected = lax.psum_scatter(
        jnp.dot(normed, joined, preferred_element_type=jnp.float32),
        "kv",
        scatter_dimension=0,
        tiled=True,
    )
    gate_z = projected[:, :inner_width].astype(jnp.bfloat16)
    x_new = projected[:, inner_width : 2 * inner_width].astype(jnp.bfloat16)
    bc_end = 2 * inner_width + 2 * group_width
    bc_new = (
        projected[:, 2 * inner_width : bc_end]
        .astype(jnp.bfloat16)
        .reshape(own_seqs, 2, group_width)
    )
    rate_raw = projected[:, bc_end:]
    full_x = jnp.concatenate([window_x, x_new[:, None]], axis=1)
    full_bc = jnp.concatenate([window_bc, bc_new[:, None]], axis=1)
    mixed_x = jax.nn.silu(
        jnp.einsum("sji,ji->si", full_x.astype(jnp.float32), conv_x.astype(jnp.float32))
    )
    mixed_bc = jax.nn.silu(
        jnp.einsum("sjci,jci->sci", full_bc.astype(jnp.float32), conv_bc.astype(jnp.float32))
    )
    heads = proj_dt.shape[1]
    state_size = ssm_state.shape[3]
    groups = group_width // state_size
    head_dim = inner_width // heads
    repeat = heads // groups
    inputs_x = mixed_x.reshape(own_seqs, heads, head_dim)
    keys_b = jnp.repeat(mixed_bc[:, 0].reshape(own_seqs, groups, state_size), repeat, axis=1)
    reads_c = jnp.repeat(mixed_bc[:, 1].reshape(own_seqs, groups, state_size), repeat, axis=1)
    step_size = jax.nn.softplus(rate_raw + dt_bias)
    retain = jnp.exp(-step_size * jnp.exp(log_rate))
    new_state = (
        retain[:, :, None, None] * ssm_state
        + (step_size[:, :, None] * inputs_x)[:, :, :, None] * keys_b[:, :, None, :]
    )
    readout = jnp.einsum("shpn,shn->shp", new_state, reads_c) + skip_gain[None, :, None] * inputs_x
    gated = readout.reshape(own_seqs, inner_width) * jax.nn.silu(gate_z.astype(jnp.float32))
    grouped = gated.reshape(own_seqs, groups, inner_width // groups)
    grouped = grouped * lax.rsqrt(jnp.mean(grouped * grouped, axis=-1, keepdims=True) + EPS)
    mixed = (grouped.reshape(own_seqs, inner_width) * group_gain).astype(jnp.bfloat16)
    partial_out = jnp.dot(
        lax.all_gather(mixed, "kv", axis=0, tiled=True),
        out_weight,
        preferred_element_type=jnp.float32,
    )
    summed_out = lax.psum_scatter(
        partial_out.astype(jnp.bfloat16), "tp", scatter_dimension=1, tiled=True
    ).astype(jnp.float32)
    after_mixer = (after_first.astype(jnp.float32) + summed_out).astype(jnp.bfloat16)
    result = half_mlp(after_mixer, mlp2_gain, mlp2_gate, mlp2_up, mlp2_down)
    return (result, new_state, full_x[:, 1:], full_bc[:, 1:])


MESH = pl.DeviceIdType.MESH
F32 = jnp.float32
BF16 = jnp.bfloat16
TOKENS, SUM1, PROJ, EXTRA, FIRST, MIXED, OUT, SUM2 = range(8)
PHASES = 8


def dot32(left, right):
    return jnp.dot(left, right, preferred_element_type=F32)


def dot32_rows(left, right):
    return lax.dot_general(left, right, (((1,), (1,)), ((), ())), preferred_element_type=F32)


def fused_kernel(
    n_kv,
    n_tp,
    tokens,
    gain1,
    gate1,
    up1,
    down1,
    gain_m,
    proj_z,
    proj_x,
    proj_bc,
    proj_dt,
    conv_x,
    conv_bc,
    window_x,
    window_bc,
    state,
    dt_bias,
    log_rate,
    skip_gain,
    group_gain,
    out_weight,
    gain2,
    gate2,
    up2,
    down2,
    result,
    step_x_out,
    retain_out,
    b_out,
    new_x_out,
    new_bc_out,
    tok_v,
    gain1_v,
    gate1_v,
    up1_v,
    down1_v,
    gain_m_v,
    z_v,
    x_v,
    bc_v,
    dt_v,
    conv_x_v,
    conv_bc_v,
    window_x_v,
    window_bc_v,
    state_v,
    bias_v,
    log_v,
    skip_v,
    ggain_v,
    out_v,
    gain2_v,
    gate2_v,
    up2_v,
    down2_v,
    state_half,
    bc_halves,
    tok_all,
    sum1_send,
    sum1_all,
    proj_send,
    proj_all,
    extra_send,
    extra_all,
    first_all,
    mixed_all,
    out_all,
    sum2_send,
    sum2_all,
    local_sem,
    send_sem,
    recv_sem,
):
    n = n_kv * n_tp
    kv, tp = lax.axis_index("kv"), lax.axis_index("tp")
    me = kv * n_tp + tp
    rows, cols = tok_v.shape
    width = cols * n
    kv_cols = cols * n_tp
    used = [0]

    def load(source, target):
        copy = pltpu.make_async_copy(source, target, local_sem.at[used[0]])
        used[0] += 1
        copy.start()
        return copy

    chunk = cols
    tok_copies = [load(tokens, tok_v), load(gain1, gain1_v)]
    gu1 = []
    for i in range(n):
        part = pl.ds(i * chunk, chunk)
        gu1.append(
            (load(gate1.at[:, part], gate1_v.at[:, part]), load(up1.at[:, part], up1_v.at[:, part]))
        )
    down1_copy = load(down1, down1_v)
    proj_copies = [
        load(gain_m, gain_m_v),
        load(proj_z, z_v),
        load(proj_x, x_v),
        load(proj_bc, bc_v),
        load(proj_dt, dt_v),
    ]
    ssm_copies = [
        load(conv_x, conv_x_v),
        load(conv_bc, conv_bc_v),
        load(window_x, window_x_v),
        load(window_bc, window_bc_v),
        load(dt_bias, bias_v),
        load(log_rate, log_v),
        load(skip_gain, skip_v),
        load(group_gain, ggain_v),
        load(state, state_v),
    ]
    out_copy = load(out_weight, out_v)
    gain2_copy = load(gain2, gain2_v)
    gu2 = [load(gate2, gate2_v), load(up2, up2_v)]
    down2_copy = load(down2, down2_v)

    def peer_of(offset):
        peer = lax.rem(me + offset, n)
        return peer, lax.div(peer, n_tp), lax.rem(peer, n_tp)

    barrier = pltpu.get_barrier_semaphore()
    for offset in range(1, n):
        _, peer_kv, peer_tp = peer_of(offset)
        pl.semaphore_signal(
            barrier, inc=1, device_id={"kv": peer_kv, "tp": peer_tp}, device_id_type=MESH
        )
    pl.semaphore_wait(barrier, n - 1)

    sends = []

    def send(source, target, phase, slot, source_slot, to_kv, to_tp):
        copy = pltpu.make_async_remote_copy(
            src_ref=source,
            dst_ref=target,
            send_sem=send_sem.at[phase, slot],
            recv_sem=recv_sem.at[phase, source_slot],
            device_id={"kv": to_kv, "tp": to_tp},
            device_id_type=MESH,
        )
        copy.start()
        sends.append(copy)

    def arrive(target, phase, source_slot):
        pltpu.make_async_remote_copy(
            src_ref=target,
            dst_ref=target,
            send_sem=send_sem.at[phase, 0],
            recv_sem=recv_sem.at[phase, source_slot],
            device_id={"kv": kv, "tp": tp},
            device_id_type=MESH,
        ).wait_recv()

    for copy in tok_copies:
        copy.wait()
    for offset in range(1, n):
        _, peer_kv, peer_tp = peer_of(offset)
        send(tok_v, tok_all.at[me], TOKENS, offset, me, peer_kv, peer_tp)
    tok_all[me] = tok_v[...]
    for offset in range(1, n):
        peer, _, _ = peer_of(offset)
        arrive(tok_all.at[peer], TOKENS, peer)

    def hidden_of(parts, gain_ref, gate_ref, up_ref, ready):
        squares = sum(jnp.sum(v * v, axis=1, keepdims=True) for v in parts)
        factor = lax.rsqrt(squares / width + EPS)
        gate_part = up_part = None
        for i, v in enumerate(parts):
            piece = v.shape[1]
            part = pl.ds(i * piece, piece)
            normed = (v * factor * gain_ref[:, part]).astype(BF16)
            ready(i)
            a, b = dot32_rows(normed, gate_ref[:, part]), dot32_rows(normed, up_ref[:, part])
            gate_part = a if i == 0 else gate_part + a
            up_part = b if i == 0 else up_part + b
        return (jax.nn.silu(gate_part) * up_part).astype(BF16)

    def ready1(i):
        for copy in gu1[i]:
            copy.wait()

    hidden1 = hidden_of(
        [tok_all[i].astype(F32) for i in range(n)], gain1_v, gate1_v, up1_v, ready1
    )
    down1_copy.wait()
    for step in range(1, n_kv + 1):
        to_kv = lax.rem(kv + step, n_kv)
        part = pl.ds(pl.multiple_of(to_kv * kv_cols, 128), kv_cols)
        partial_sum = dot32(hidden1, down1_v[:, part]).astype(BF16)
        if step < n_kv:
            sum1_send[step] = partial_sum
            for other in range(n_tp):
                to_tp = lax.rem(tp + other, n_tp)
                send(
                    sum1_send.at[step],
                    sum1_all.at[me],
                    SUM1,
                    step * n_tp + other,
                    me,
                    to_kv,
                    to_tp,
                )
        else:
            sum1_all[me] = partial_sum
            sum1_send[0] = partial_sum
            for other in range(1, n_tp):
                to_tp = lax.rem(tp + other, n_tp)
                send(sum1_send.at[0], sum1_all.at[me], SUM1, other, me, kv, to_tp)

    for copy in ssm_copies:
        copy.wait()
    seqs = window_x_v.shape[1]
    state_size = state_v.shape[2]
    heads = dt_v.shape[0]
    inner = z_v.shape[1]
    group_width = bc_v.shape[2]
    groups = group_width // state_size
    head_dim = inner // heads
    group_inner = inner // groups
    taps = conv_x_v.shape[0]
    conv_xf = conv_x_v[...].astype(F32)
    past_x = sum(window_x_v[j].astype(F32) * conv_xf[j : j + 1] for j in range(taps - 1))
    past_pairs = [
        sum(window_bc_v[s, j].astype(F32) * conv_bc_v[j].astype(F32) for j in range(taps - 1))
        for s in range(seqs)
    ]

    def side_by_side(pairs):
        return jnp.concatenate(
            [jnp.concatenate([p[h : h + 1] for p in pairs], axis=0) for h in range(2)], axis=1
        )

    past_bc = side_by_side(past_pairs)
    last_bc = side_by_side([conv_bc_v[taps - 1].astype(F32)])
    for j in range(1, taps - 1):
        new_x_out[j - 1] = window_x_v[j]
        for s in range(seqs):
            new_bc_out[s, j - 1] = window_bc_v[s, j]
    state_half[...] = state_v[...].astype(BF16)
    lanes = lax.broadcasted_iota(jnp.int32, (heads, inner), 1)
    owner = lax.broadcasted_iota(jnp.int32, (heads, inner), 0)
    low = owner * head_dim
    spread = jnp.where((lanes >= low) & (lanes < low + head_dim), 1.0, 0.0).astype(F32)

    def expand(values):
        return jnp.dot(
            values, spread, preferred_element_type=F32, precision=lax.Precision.HIGHEST
        )

    skip = expand(jnp.broadcast_to(skip_v[...], (8, heads)))[:seqs]
    for copy in proj_copies:
        copy.wait()
    for half in range(2):
        bc_halves[half] = bc_v[:, half, :]

    for offset in range(1, n):
        peer, _, _ = peer_of(offset)
        arrive(sum1_all.at[peer], SUM1, peer)
    summed = sum1_all[0].astype(F32)
    for i in range(1, n):
        summed = summed + sum1_all[i].astype(F32)
    base = jnp.concatenate([tok_all[kv * n_tp + t].astype(F32) for t in range(n_tp)], axis=1)
    after = (base + 0.5 * summed).astype(BF16)
    first_all[kv] = after
    after32 = after.astype(F32)
    squares = jnp.sum(after32 * after32, axis=1, keepdims=True)
    gain_part = gain_m_v[:, pl.ds(pl.multiple_of(kv * kv_cols, 128), kv_cols)]
    scaled = (after32 * gain_part).astype(BF16)
    own_rates = dot32_rows(scaled, dt_v[...])
    for k in range(n_kv):
        rows_k = slice(k * seqs, (k + 1) * seqs)
        extra_send[k] = jnp.broadcast_to(squares[rows_k], (seqs, extra_send.shape[2]))
        extra_send[k, :, :heads] = own_rates[rows_k]
    for place, weight in (
        (0, z_v),
        (inner, x_v),
        (2 * inner, bc_halves.at[0]),
        (2 * inner + group_width, bc_halves.at[1]),
    ):
        piece = dot32(scaled, weight[...])
        for k in range(n_kv):
            proj_send[k, :, pl.ds(place, weight.shape[1])] = piece[
                k * seqs : (k + 1) * seqs
            ].astype(BF16)
    proj_all[kv] = proj_send[kv]
    extra_all[kv] = extra_send[kv]
    for step in range(1, n_kv):
        to_kv = lax.rem(kv + step, n_kv)
        send(proj_send.at[to_kv], proj_all.at[kv], PROJ, step, kv, to_kv, tp)
        send(extra_send.at[to_kv], extra_all.at[kv], EXTRA, step, kv, to_kv, tp)
    for step in range(1, n_kv):
        to_kv = lax.rem(kv + step, n_kv)
        send(first_all.at[kv], first_all.at[kv], FIRST, step, kv, to_kv, tp)

    for step in range(1, n_kv):
        from_kv = lax.rem(kv + step, n_kv)
        arrive(extra_all.at[from_kv], EXTRA, from_kv)
        arrive(proj_all.at[from_kv], PROJ, from_kv)
    extra = extra_all[0]
    projected = proj_all[0].astype(F32)
    for k in range(1, n_kv):
        extra = extra + extra_all[k]
        projected = projected + proj_all[k].astype(F32)
    factor = lax.rsqrt(extra[:, heads : heads + 1] / width + EPS)
    projected = projected * factor
    step_size = extra[:, :heads] * factor + bias_v[...]
    step_size = jnp.maximum(step_size, 0.0) + jnp.log1p(jnp.exp(-jnp.abs(step_size)))
    retain = jnp.exp(-step_size * jnp.exp(log_v[...]))
    gate_z = projected[:, :inner].astype(BF16).astype(F32)
    x_new = projected[:, inner : 2 * inner].astype(BF16)
    bc_new = projected[:, 2 * inner :].astype(BF16)
    mixed_x = jax.nn.silu(past_x + conv_xf[taps - 1 :] * x_new.astype(F32))
    mixed_bc = jax.nn.silu(past_bc + last_bc * bc_new.astype(F32))
    step_x = expand(step_size) * mixed_x
    retained = expand(retain)
    pieces = []
    which = lax.broadcasted_iota(jnp.int32, (seqs, group_inner), 0)
    for g in range(groups):
        b = mixed_bc[:, g * state_size : (g + 1) * state_size]
        c = mixed_bc[:, group_width + g * state_size : group_width + (g + 1) * state_size]
        span = slice(g * group_inner, (g + 1) * group_inner)
        old = None
        for s in range(seqs):
            read = lax.dot_general(
                c.astype(BF16),
                state_half[s, g * group_inner : (g + 1) * group_inner, :],
                (((1,), (1,)), ((), ())),
                preferred_element_type=F32,
            )
            old = read if s == 0 else jnp.where(which == s, read, old)
        match = jnp.sum(b * c, axis=1, keepdims=True)
        readout = retained[:, span] * old + step_x[:, span] * match + skip[:, span] * mixed_x[:, span]
        z = gate_z[:, span]
        gated = readout * jax.nn.silu(z)
        gated = gated * lax.rsqrt(jnp.mean(gated * gated, axis=1, keepdims=True) + EPS)
        pieces.append((gated * ggain_v[:, span]).astype(BF16))
    mixed_all[kv] = jnp.concatenate(pieces, axis=1)
    for step in range(1, n_kv):
        to_kv = lax.rem(kv + step, n_kv)
        send(mixed_all.at[kv], mixed_all.at[kv], MIXED, step, kv, to_kv, tp)
    step_x_out[...] = step_x
    retain_out[...] = retained
    b_out[...] = mixed_bc[:, :group_width]
    new_x_out[taps - 2] = x_new
    bc32 = bc_new.astype(F32)
    for s in range(seqs):
        new_bc_out[s, taps - 2] = jnp.concatenate(
            [bc32[s : s + 1, :group_width], bc32[s : s + 1, group_width:]], axis=0
        ).astype(BF16)
    out_copy.wait()
    for step in range(1, n_kv):
        from_kv = lax.rem(kv + step, n_kv)
        arrive(mixed_all.at[from_kv], MIXED, from_kv)
    mixed = jnp.concatenate([mixed_all[k].astype(F32) for k in range(n_kv)], axis=0)
    out_all[me] = dot32(mixed.astype(BF16), out_v[...]).astype(BF16)
    for offset in range(1, n):
        _, peer_kv, peer_tp = peer_of(offset)
        send(out_all.at[me], out_all.at[me], OUT, offset, me, peer_kv, peer_tp)

    gain2_copy.wait()
    for copy in gu2:
        copy.wait()
    down2_copy.wait()
    for step in range(1, n_kv):
        from_kv = lax.rem(kv + step, n_kv)
        arrive(first_all.at[from_kv], FIRST, from_kv)
    for offset in range(1, n):
        peer, _, _ = peer_of(offset)
        arrive(out_all.at[peer], OUT, peer)

    def after_of(k):
        total = out_all[k * n_tp].astype(F32)
        for t in range(1, n_tp):
            total = total + out_all[k * n_tp + t].astype(F32)
        return (first_all[k].astype(F32) + total).astype(BF16).astype(F32)

    hidden2 = hidden_of(
        [after_of(k) for k in range(n_kv)], gain2_v, gate2_v, up2_v, lambda i: None
    )
    for offset in range(1, n + 1):
        peer, peer_kv, peer_tp = peer_of(offset)
        part = pl.ds(pl.multiple_of(peer * cols, 128), cols)
        partial_sum = dot32(hidden2, down2_v[:, part]).astype(BF16)
        if offset < n:
            sum2_send[offset] = partial_sum
            send(sum2_send.at[offset], sum2_all.at[me], SUM2, offset, me, peer_kv, peer_tp)
        else:
            sum2_all[me] = partial_sum
    own = after_of(kv)
    mine = own[:, :cols]
    for t in range(1, n_tp):
        mine = jnp.where(tp == t, own[:, t * cols : (t + 1) * cols], mine)
    for offset in range(1, n):
        peer, _, _ = peer_of(offset)
        arrive(sum2_all.at[peer], SUM2, peer)
    summed = sum2_all[0].astype(F32)
    for i in range(1, n):
        summed = summed + sum2_all[i].astype(F32)
    result[...] = (mine + 0.5 * summed).astype(BF16)
    for copy in sends:
        copy.wait_send()


def finish_kernel(
    result,
    step_x,
    retain,
    keys_b,
    new_x,
    new_bc,
    state,
    result_out,
    state_out,
    new_x_out,
    new_bc_out,
    fresh,
    sems,
):
    seqs, inner, state_size = state.shape
    groups = keys_b.shape[1] // state_size
    span = inner // groups
    rows = jnp.concatenate([retain[...], step_x[...], retain[...], step_x[...]], axis=0)
    columns = rows.T
    copies = []
    for g in range(groups):
        part = slice(g * span, (g + 1) * span)
        for s in range(seqs):
            fresh[s, part, :] = (
                columns[part, s : s + 1] * state[s, part, :]
                + columns[part, seqs + s : seqs + s + 1]
                * keys_b[s : s + 1, g * state_size : (g + 1) * state_size]
            )
            copy = pltpu.make_async_copy(
                fresh.at[s, part], state_out.at[s, part], sems.at[s, g]
            )
            copy.start()
            copies.append(copy)
    result_out[...] = result[...]
    new_x_out[...] = new_x[...]
    new_bc_out[...] = new_bc[...]
    for copy in copies:
        copy.wait()


def per_device(n_kv, n_tp, *args):
    (
        tokens,
        mlp1_gain,
        mlp1_gate,
        mlp1_up,
        mlp1_down,
        mixer_gain,
        proj_z,
        proj_x,
        proj_bc,
        proj_dt,
        conv_x,
        conv_bc,
        window_x,
        window_bc,
        ssm_state,
        dt_bias,
        log_rate,
        skip_gain,
        group_gain,
        out_weight,
        mlp2_gain,
        mlp2_gate,
        mlp2_up,
        mlp2_down,
    ) = args
    rows, cols = tokens.shape
    if cols % 128 or n_kv * n_tp > 16 or rows % 8:
        return plain_device(*args)
    n = n_kv * n_tp
    kv_cols = cols * n_tp
    seqs, heads = window_x.shape[0], proj_dt.shape[1]
    inner, group_width = proj_z.shape[1], proj_bc.shape[2]
    state_size = ssm_state.shape[3]
    groups = group_width // state_size
    taps = conv_x.shape[0]
    operands = (
        tokens,
        mlp1_gain[None],
        mlp1_gate.T,
        mlp1_up.T,
        mlp1_down,
        mixer_gain[None],
        proj_z,
        proj_x,
        proj_bc,
        proj_dt.T,
        conv_x,
        conv_bc,
        jnp.swapaxes(window_x, 0, 1),
        window_bc,
        ssm_state.reshape(seqs, inner, state_size),
        dt_bias[None],
        log_rate[None],
        skip_gain[None],
        group_gain[None],
        out_weight,
        mlp2_gain[None],
        mlp2_gate.T,
        mlp2_up.T,
        mlp2_down,
    )
    vmem = [pltpu.VMEM(a.shape, a.dtype) for a in operands]
    scratch = vmem + [
        pltpu.VMEM((seqs, inner, state_size), BF16),
        pltpu.VMEM((2, proj_bc.shape[0], group_width), BF16),
        pltpu.VMEM((n, rows, cols), BF16),
        pltpu.VMEM((n_kv, rows, kv_cols), BF16),
        pltpu.VMEM((n, rows, kv_cols), BF16),
        pltpu.VMEM((n_kv, seqs, 2 * inner + 2 * group_width), BF16),
        pltpu.VMEM((n_kv, seqs, 2 * inner + 2 * group_width), BF16),
        pltpu.VMEM((n_kv, seqs, 128), F32),
        pltpu.VMEM((n_kv, seqs, 128), F32),
        pltpu.VMEM((n_kv, rows, kv_cols), BF16),
        pltpu.VMEM((n_kv, seqs, inner), BF16),
        pltpu.VMEM((n, rows, kv_cols), BF16),
        pltpu.VMEM((n, rows, cols), BF16),
        pltpu.VMEM((n, rows, cols), BF16),
        pltpu.SemaphoreType.DMA((2 * n + 40,)),
        pltpu.SemaphoreType.DMA((PHASES, n)),
        pltpu.SemaphoreType.DMA((PHASES, n)),
    ]
    shapes = (
        jax.ShapeDtypeStruct((rows, cols), BF16),
        jax.ShapeDtypeStruct((seqs, inner), F32),
        jax.ShapeDtypeStruct((seqs, inner), F32),
        jax.ShapeDtypeStruct((seqs, group_width), F32),
        jax.ShapeDtypeStruct((taps - 1, seqs, inner), BF16),
        jax.ShapeDtypeStruct(window_bc.shape, BF16),
    )
    result, step_x, retain, keys_b, new_x, new_bc = pl.pallas_call(
        functools.partial(fused_kernel, n_kv, n_tp),
        out_shape=shapes,
        in_specs=[pl.BlockSpec(memory_space=pl.ANY)] * len(operands),
        out_specs=[pl.BlockSpec(memory_space=pltpu.VMEM)] * len(shapes),
        scratch_shapes=scratch,
        compiler_params=pltpu.CompilerParams(
            collective_id=0, has_side_effects=True, vmem_limit_bytes=60 * 1024 * 1024
        ),
    )(*operands)
    whole = pl.BlockSpec(memory_space=pltpu.VMEM)
    result, new_state, new_x, new_bc = pl.pallas_call(
        finish_kernel,
        out_shape=(
            shapes[0],
            jax.ShapeDtypeStruct(operands[14].shape, F32),
            shapes[4],
            shapes[5],
        ),
        in_specs=[whole] * 7,
        out_specs=(whole, pl.BlockSpec(memory_space=pl.ANY), whole, whole),
        scratch_shapes=[
            pltpu.VMEM(operands[14].shape, F32),
            pltpu.SemaphoreType.DMA((seqs, groups)),
        ],
    )(result, step_x, retain, keys_b, new_x, new_bc, operands[14])
    return (result, new_state.reshape(ssm_state.shape), jnp.swapaxes(new_x, 0, 1), new_bc)


def solution(mesh):
    placed = (
        P("dp", ("kv", "tp")),
        P(),
        P(None, ("kv", "tp")),
        P(None, ("kv", "tp")),
        P(("kv", "tp"), None),
        P(),
        P("kv", "tp"),
        P("kv", "tp"),
        P("kv", None, "tp"),
        P("kv", "tp"),
        P(None, "tp"),
        P(None, None, "tp"),
        P(("dp", "kv"), None, "tp"),
        P(("dp", "kv"), None, None, "tp"),
        P(("dp", "kv"), "tp", None, None),
        P("tp"),
        P("tp"),
        P("tp"),
        P("tp"),
        P("tp", "kv"),
        P(),
        P(None, ("kv", "tp")),
        P(None, ("kv", "tp")),
        P(("kv", "tp"), None),
    )
    return jax.shard_map(
        functools.partial(per_device, mesh.shape["kv"], mesh.shape["tp"]),
        mesh=mesh,
        in_specs=placed,
        out_specs=(
            P("dp", ("kv", "tp")),
            P(("dp", "kv"), "tp", None, None),
            P(("dp", "kv"), None, "tp"),
            P(("dp", "kv"), None, None, "tp"),
        ),
        check_vma=False,
    )
```

```python
import functools

import jax
import jax.numpy as jnp
from jax import lax
from jax.experimental import pallas as pl
from jax.experimental.pallas import tpu as pltpu
from jax.sharding import PartitionSpec as P

EPS = 1e-06


def norm_rows(values, scale_gain):
    floats = values.astype(jnp.float32)
    factor = lax.rsqrt(jnp.mean(floats * floats, axis=-1, keepdims=True) + EPS)
    return (floats * factor * scale_gain).astype(jnp.bfloat16)


def half_mlp(columns, scale_gain, gate_weight, up_weight, down_weight):
    gathered = lax.all_gather(columns, ("kv", "tp"), axis=1, tiled=True)
    normed = norm_rows(gathered, scale_gain)
    gate_part = jnp.dot(normed, gate_weight, preferred_element_type=jnp.float32)
    up_part = jnp.dot(normed, up_weight, preferred_element_type=jnp.float32)
    hidden = (jax.nn.silu(gate_part) * up_part).astype(jnp.bfloat16)
    partial_sums = jnp.dot(hidden, down_weight, preferred_element_type=jnp.float32)
    summed = lax.psum_scatter(partial_sums, ("kv", "tp"), scatter_dimension=1, tiled=True)
    return (columns.astype(jnp.float32) + 0.5 * summed).astype(jnp.bfloat16)


def plain_device(
    tokens,
    mlp1_gain,
    mlp1_gate,
    mlp1_up,
    mlp1_down,
    mixer_gain,
    proj_z,
    proj_x,
    proj_bc,
    proj_dt,
    conv_x,
    conv_bc,
    window_x,
    window_bc,
    ssm_state,
    dt_bias,
    log_rate,
    skip_gain,
    group_gain,
    out_weight,
    mlp2_gain,
    mlp2_gate,
    mlp2_up,
    mlp2_down,
):
    after_first = half_mlp(tokens, mlp1_gain, mlp1_gate, mlp1_up, mlp1_down)
    kv_width = proj_z.shape[0]
    kv_offset = lax.axis_index("kv") * kv_width
    gathered = lax.all_gather(after_first, ("kv", "tp"), axis=1, tiled=True)
    floats = gathered.astype(jnp.float32)
    squares = jnp.sum(floats * floats, axis=1)
    own_cols = lax.dynamic_slice_in_dim(gathered, kv_offset, kv_width, 1)
    model_width = kv_width * lax.axis_size("kv")
    factor = lax.rsqrt(squares / model_width + EPS)
    gain_cols = lax.dynamic_slice_in_dim(mixer_gain, kv_offset, kv_width, 0)
    normed = (own_cols.astype(jnp.float32) * factor[:, None] * gain_cols).astype(jnp.bfloat16)
    inner_width = proj_z.shape[1]
    group_width = proj_bc.shape[2]
    joined = jnp.concatenate(
        [proj_z, proj_x, proj_bc.reshape(kv_width, 2 * group_width), proj_dt], axis=1
    )
    own_seqs = window_x.shape[0]
    projected = lax.psum_scatter(
        jnp.dot(normed, joined, preferred_element_type=jnp.float32),
        "kv",
        scatter_dimension=0,
        tiled=True,
    )
    gate_z = projected[:, :inner_width].astype(jnp.bfloat16)
    x_new = projected[:, inner_width : 2 * inner_width].astype(jnp.bfloat16)
    bc_end = 2 * inner_width + 2 * group_width
    bc_new = (
        projected[:, 2 * inner_width : bc_end]
        .astype(jnp.bfloat16)
        .reshape(own_seqs, 2, group_width)
    )
    rate_raw = projected[:, bc_end:]
    full_x = jnp.concatenate([window_x, x_new[:, None]], axis=1)
    full_bc = jnp.concatenate([window_bc, bc_new[:, None]], axis=1)
    mixed_x = jax.nn.silu(
        jnp.einsum("sji,ji->si", full_x.astype(jnp.float32), conv_x.astype(jnp.float32))
    )
    mixed_bc = jax.nn.silu(
        jnp.einsum("sjci,jci->sci", full_bc.astype(jnp.float32), conv_bc.astype(jnp.float32))
    )
    heads = proj_dt.shape[1]
    state_size = ssm_state.shape[3]
    groups = group_width // state_size
    head_dim = inner_width // heads
    repeat = heads // groups
    inputs_x = mixed_x.reshape(own_seqs, heads, head_dim)
    keys_b = jnp.repeat(mixed_bc[:, 0].reshape(own_seqs, groups, state_size), repeat, axis=1)
    reads_c = jnp.repeat(mixed_bc[:, 1].reshape(own_seqs, groups, state_size), repeat, axis=1)
    step_size = jax.nn.softplus(rate_raw + dt_bias)
    retain = jnp.exp(-step_size * jnp.exp(log_rate))
    new_state = (
        retain[:, :, None, None] * ssm_state
        + (step_size[:, :, None] * inputs_x)[:, :, :, None] * keys_b[:, :, None, :]
    )
    readout = jnp.einsum("shpn,shn->shp", new_state, reads_c) + skip_gain[None, :, None] * inputs_x
    gated = readout.reshape(own_seqs, inner_width) * jax.nn.silu(gate_z.astype(jnp.float32))
    grouped = gated.reshape(own_seqs, groups, inner_width // groups)
    grouped = grouped * lax.rsqrt(jnp.mean(grouped * grouped, axis=-1, keepdims=True) + EPS)
    mixed = (grouped.reshape(own_seqs, inner_width) * group_gain).astype(jnp.bfloat16)
    partial_out = jnp.dot(
        lax.all_gather(mixed, "kv", axis=0, tiled=True),
        out_weight,
        preferred_element_type=jnp.float32,
    )
    summed_out = lax.psum_scatter(
        partial_out.astype(jnp.bfloat16), "tp", scatter_dimension=1, tiled=True
    ).astype(jnp.float32)
    after_mixer = (after_first.astype(jnp.float32) + summed_out).astype(jnp.bfloat16)
    result = half_mlp(after_mixer, mlp2_gain, mlp2_gate, mlp2_up, mlp2_down)
    return (result, new_state, full_x[:, 1:], full_bc[:, 1:])


MESH = pl.DeviceIdType.MESH
F32 = jnp.float32
BF16 = jnp.bfloat16
TOKENS, SUM1, PROJ, EXTRA, FIRST, MIXED, OUT, SUM2 = range(8)
PHASES = 8


def dot32(left, right):
    return jnp.dot(left, right, preferred_element_type=F32)


def dot32_rows(left, right):
    return lax.dot_general(left, right, (((1,), (1,)), ((), ())), preferred_element_type=F32)


def fused_kernel(
    n_kv,
    n_tp,
    tokens,
    gain1,
    gate1,
    up1,
    down1,
    gain_m,
    proj_z,
    proj_x,
    proj_bc,
    proj_dt,
    conv_x,
    conv_bc,
    window_x,
    window_bc,
    state,
    dt_bias,
    log_rate,
    skip_gain,
    group_gain,
    out_weight,
    gain2,
    gate2,
    up2,
    down2,
    result,
    step_x_out,
    retain_out,
    b_out,
    new_x_out,
    new_bc_out,
    tok_v,
    gain1_v,
    gate1_v,
    up1_v,
    down1_v,
    gain_m_v,
    z_v,
    x_v,
    bc_v,
    dt_v,
    conv_x_v,
    conv_bc_v,
    window_x_v,
    window_bc_v,
    state_v,
    bias_v,
    log_v,
    skip_v,
    ggain_v,
    out_v,
    gain2_v,
    gate2_v,
    up2_v,
    down2_v,
    state_half,
    bc_halves,
    tok_all,
    sum1_send,
    sum1_all,
    proj_send,
    proj_all,
    extra_send,
    extra_all,
    first_all,
    mixed_all,
    out_all,
    sum2_send,
    sum2_all,
    result_v,
    step_x_v,
    retain_v,
    b_v,
    new_x_v,
    new_bc_v,
    local_sem,
    send_sem,
    recv_sem,
):
    n = n_kv * n_tp
    kv, tp = lax.axis_index("kv"), lax.axis_index("tp")
    me = kv * n_tp + tp
    rows, cols = tok_v.shape
    width = cols * n
    kv_cols = cols * n_tp
    used = [0]

    def load(source, target):
        copy = pltpu.make_async_copy(source, target, local_sem.at[used[0]])
        used[0] += 1
        copy.start()
        return copy

    def nth_kv(i):
        down = n_kv - 1 - i
        down = down - lax.div(kv - down + n_kv, n_kv)
        up = i + lax.div(i - kv + n_kv, n_kv)
        half = lax.div(2 * kv, n_kv)
        return down * (1 - half) + up * half

    far_kv = [nth_kv(i) for i in range(n_kv - 1)]
    others_tp = [lax.rem(tp + t, n_tp) for t in range(1, n_tp)]
    all_tp = [tp] + others_tp
    far_peers = [(k, t) for k in far_kv for t in all_tp] + [(kv, t) for t in others_tp]
    near_first = [(kv, tp)] + far_peers[::-1]

    tok_copies = [load(tokens, tok_v), load(gain1, gain1_v)]
    gu1 = []
    for k, t in near_first:
        part = pl.ds(pl.multiple_of((k * n_tp + t) * cols, 128), cols)
        gu1.append(
            (load(gate1.at[:, part], gate1_v.at[:, part]), load(up1.at[:, part], up1_v.at[:, part]))
        )
    down1_copy = load(down1, down1_v)
    proj_copies = [
        load(gain_m, gain_m_v),
        load(proj_z, z_v),
        load(proj_x, x_v),
        load(proj_bc, bc_v),
        load(proj_dt, dt_v),
    ]
    ssm_copies = [
        load(conv_x, conv_x_v),
        load(conv_bc, conv_bc_v),
        load(window_x, window_x_v),
        load(window_bc, window_bc_v),
        load(dt_bias, bias_v),
        load(log_rate, log_v),
        load(skip_gain, skip_v),
        load(group_gain, ggain_v),
        load(state, state_v),
    ]
    out_copy = load(out_weight, out_v)
    gain2_copy = load(gain2, gain2_v)
    gu2 = [load(gate2, gate2_v), load(up2, up2_v)]
    down2_copy = load(down2, down2_v)

    barrier = pltpu.get_barrier_semaphore()
    for k, t in far_peers:
        pl.semaphore_signal(barrier, inc=1, device_id={"kv": k, "tp": t}, device_id_type=MESH)
    pl.semaphore_wait(barrier, n - 1)

    sends = []

    def send(source, target, phase, slot, source_slot, to_kv, to_tp):
        copy = pltpu.make_async_remote_copy(
            src_ref=source,
            dst_ref=target,
            send_sem=send_sem.at[phase, slot],
            recv_sem=recv_sem.at[phase, source_slot],
            device_id={"kv": to_kv, "tp": to_tp},
            device_id_type=MESH,
        )
        copy.start()
        sends.append(copy)

    def arrive(target, phase, source_slot):
        pltpu.make_async_remote_copy(
            src_ref=target,
            dst_ref=target,
            send_sem=send_sem.at[phase, 0],
            recv_sem=recv_sem.at[phase, source_slot],
            device_id={"kv": kv, "tp": tp},
            device_id_type=MESH,
        ).wait_recv()

    for copy in tok_copies:
        copy.wait()
    for i, (k, t) in enumerate(far_peers):
        send(tok_v, tok_all.at[me], TOKENS, i, me, k, t)
    tok_all[me] = tok_v[...]

    def hidden_of(sources, value_of, gain_ref, gate_ref, up_ref):
        squares = gate_part = up_part = None
        for i, source in enumerate(sources):
            index, v = value_of(i, source)
            piece = v.shape[1]
            part = pl.ds(pl.multiple_of(index * piece, 128), piece)
            scaled_v = (v * gain_ref[:, part]).astype(BF16)
            q = jnp.sum(v * v, axis=1, keepdims=True)
            a = dot32_rows(scaled_v, gate_ref[:, part])
            b = dot32_rows(scaled_v, up_ref[:, part])
            squares = q if i == 0 else squares + q
            gate_part = a if i == 0 else gate_part + a
            up_part = b if i == 0 else up_part + b
        factor = lax.rsqrt(squares / width + EPS)
        return (jax.nn.silu(gate_part * factor) * (up_part * factor)).astype(BF16)

    def token_block(i, source):
        peer = source[0] * n_tp + source[1]
        if i:
            arrive(tok_all.at[peer], TOKENS, peer)
        for copy in gu1[i]:
            copy.wait()
        return peer, (tok_all[peer] if i else tok_v[...]).astype(F32)

    hidden1 = hidden_of(near_first, token_block, gain1_v, gate1_v, up1_v)
    down1_copy.wait()
    for i, to_kv in enumerate(far_kv + [kv]):
        part = pl.ds(pl.multiple_of(to_kv * kv_cols, 128), kv_cols)
        partial_sum = dot32(hidden1, down1_v[:, part]).astype(BF16)
        sum1_send[i] = partial_sum
        if i == n_kv - 1:
            sum1_all[me] = partial_sum
        for j, to_tp in enumerate(all_tp):
            if i < n_kv - 1 or j:
                send(sum1_send.at[i], sum1_all.at[me], SUM1, i * n_tp + j, me, to_kv, to_tp)

    for copy in ssm_copies:
        copy.wait()
    seqs = window_x_v.shape[1]
    state_size = state_v.shape[2]
    heads = dt_v.shape[0]
    inner = z_v.shape[1]
    group_width = bc_v.shape[2]
    groups = group_width // state_size
    head_dim = inner // heads
    group_inner = inner // groups
    taps = conv_x_v.shape[0]
    conv_xf = conv_x_v[...].astype(F32)
    past_x = sum(window_x_v[j].astype(F32) * conv_xf[j : j + 1] for j in range(taps - 1))
    past_pairs = [
        sum(window_bc_v[s, j].astype(F32) * conv_bc_v[j].astype(F32) for j in range(taps - 1))
        for s in range(seqs)
    ]

    def side_by_side(pairs):
        return jnp.concatenate(
            [jnp.concatenate([p[h : h + 1] for p in pairs], axis=0) for h in range(2)], axis=1
        )

    past_bc = side_by_side(past_pairs)
    last_bc = side_by_side([conv_bc_v[taps - 1].astype(F32)])
    for j in range(1, taps - 1):
        new_x_v[j - 1] = window_x_v[j]
        for s in range(seqs):
            new_bc_v[s, j - 1] = window_bc_v[s, j]
    state_half[...] = state_v[...].astype(BF16)
    lanes = lax.broadcasted_iota(jnp.int32, (heads, inner), 1)
    owner = lax.broadcasted_iota(jnp.int32, (heads, inner), 0)
    low = owner * head_dim
    spread = jnp.where((lanes >= low) & (lanes < low + head_dim), 1.0, 0.0).astype(F32)

    def expand(values):
        return jnp.dot(
            values, spread, preferred_element_type=F32, precision=lax.Precision.HIGHEST
        )

    skip = expand(jnp.broadcast_to(skip_v[...], (8, heads)))[:seqs]
    for copy in proj_copies:
        copy.wait()
    for half in range(2):
        bc_halves[half] = bc_v[:, half, :]

    for k, t in far_peers:
        arrive(sum1_all.at[k * n_tp + t], SUM1, k * n_tp + t)
    summed = sum1_all[0].astype(F32)
    for i in range(1, n):
        summed = summed + sum1_all[i].astype(F32)
    base = jnp.concatenate([tok_all[kv * n_tp + t].astype(F32) for t in range(n_tp)], axis=1)
    after = (base + 0.5 * summed).astype(BF16)
    first_all[kv] = after
    after32 = after.astype(F32)
    squares = jnp.sum(after32 * after32, axis=1, keepdims=True)
    gain_part = gain_m_v[:, pl.ds(pl.multiple_of(kv * kv_cols, 128), kv_cols)]
    scaled = (after32 * gain_part).astype(BF16)
    own_rates = dot32_rows(scaled, dt_v[...])
    for k in range(n_kv):
        rows_k = slice(k * seqs, (k + 1) * seqs)
        extra_send[k] = jnp.broadcast_to(squares[rows_k], (seqs, extra_send.shape[2]))
        extra_send[k, :, :heads] = own_rates[rows_k]
    for place, weight in (
        (0, z_v),
        (inner, x_v),
        (2 * inner, bc_halves.at[0]),
        (2 * inner + group_width, bc_halves.at[1]),
    ):
        piece = dot32(scaled, weight[...])
        for k in range(n_kv):
            proj_send[k, :, pl.ds(place, weight.shape[1])] = piece[
                k * seqs : (k + 1) * seqs
            ].astype(BF16)
    proj_all[kv] = proj_send[kv]
    extra_all[kv] = extra_send[kv]
    for step, to_kv in enumerate(far_kv):
        send(proj_send.at[to_kv], proj_all.at[kv], PROJ, step, kv, to_kv, tp)
        send(extra_send.at[to_kv], extra_all.at[kv], EXTRA, step, kv, to_kv, tp)
    for step, to_kv in enumerate(far_kv):
        send(first_all.at[kv], first_all.at[kv], FIRST, step, kv, to_kv, tp)

    for from_kv in far_kv:
        arrive(extra_all.at[from_kv], EXTRA, from_kv)
        arrive(proj_all.at[from_kv], PROJ, from_kv)
    extra = extra_all[0]
    projected = proj_all[0].astype(F32)
    for k in range(1, n_kv):
        extra = extra + extra_all[k]
        projected = projected + proj_all[k].astype(F32)
    factor = lax.rsqrt(extra[:, heads : heads + 1] / width + EPS)
    projected = projected * factor
    step_size = extra[:, :heads] * factor + bias_v[...]
    step_size = jnp.maximum(step_size, 0.0) + jnp.log1p(jnp.exp(-jnp.abs(step_size)))
    retain = jnp.exp(-step_size * jnp.exp(log_v[...]))
    gate_z = projected[:, :inner].astype(BF16).astype(F32)
    x_new = projected[:, inner : 2 * inner].astype(BF16)
    bc_new = projected[:, 2 * inner :].astype(BF16)
    mixed_x = jax.nn.silu(past_x + conv_xf[taps - 1 :] * x_new.astype(F32))
    mixed_bc = jax.nn.silu(past_bc + last_bc * bc_new.astype(F32))
    step_x = expand(step_size) * mixed_x
    retained = expand(retain)
    pieces = []
    which = lax.broadcasted_iota(jnp.int32, (seqs, group_inner), 0)
    for g in range(groups):
        b = mixed_bc[:, g * state_size : (g + 1) * state_size]
        c = mixed_bc[:, group_width + g * state_size : group_width + (g + 1) * state_size]
        span = slice(g * group_inner, (g + 1) * group_inner)
        old = None
        for s in range(seqs):
            read = lax.dot_general(
                c.astype(BF16),
                state_half[s, g * group_inner : (g + 1) * group_inner, :],
                (((1,), (1,)), ((), ())),
                preferred_element_type=F32,
            )
            old = read if s == 0 else jnp.where(which == s, read, old)
        match = jnp.sum(b * c, axis=1, keepdims=True)
        readout = retained[:, span] * old + step_x[:, span] * match + skip[:, span] * mixed_x[:, span]
        z = gate_z[:, span]
        gated = readout * jax.nn.silu(z)
        gated = gated * lax.rsqrt(jnp.mean(gated * gated, axis=1, keepdims=True) + EPS)
        pieces.append((gated * ggain_v[:, span]).astype(BF16))
    mixed_all[kv] = jnp.concatenate(pieces, axis=1)
    for step, to_kv in enumerate(far_kv):
        send(mixed_all.at[kv], mixed_all.at[kv], MIXED, step, kv, to_kv, tp)
    step_x_v[...] = step_x
    retain_v[...] = retained
    b_v[...] = mixed_bc[:, :group_width]
    new_x_v[taps - 2] = x_new
    bc32 = bc_new.astype(F32)
    for s in range(seqs):
        new_bc_v[s, taps - 2] = jnp.concatenate(
            [bc32[s : s + 1, :group_width], bc32[s : s + 1, group_width:]], axis=0
        ).astype(BF16)
    out_copies = [
        load(step_x_v, step_x_out),
        load(retain_v, retain_out),
        load(b_v, b_out),
        load(new_x_v, new_x_out),
        load(new_bc_v, new_bc_out),
    ]
    out_copy.wait()
    for from_kv in far_kv:
        arrive(mixed_all.at[from_kv], MIXED, from_kv)
    mixed = jnp.concatenate([mixed_all[k].astype(F32) for k in range(n_kv)], axis=0)
    out_all[me] = dot32(mixed.astype(BF16), out_v[...]).astype(BF16)
    for i, (k, t) in enumerate(far_peers):
        send(out_all.at[me], out_all.at[me], OUT, i, me, k, t)

    gain2_copy.wait()
    for copy in gu2:
        copy.wait()
    down2_copy.wait()

    def after_of(k):
        total = out_all[k * n_tp].astype(F32)
        for t in range(1, n_tp):
            total = total + out_all[k * n_tp + t].astype(F32)
        return (first_all[k].astype(F32) + total).astype(BF16).astype(F32)

    def mixer_block(i, k):
        for t in all_tp if i else others_tp:
            arrive(out_all.at[k * n_tp + t], OUT, k * n_tp + t)
        if i:
            arrive(first_all.at[k], FIRST, k)
        return k, after_of(k)

    hidden2 = hidden_of([kv] + far_kv[::-1], mixer_block, gain2_v, gate2_v, up2_v)
    for i, to_kv in enumerate(far_kv + [kv]):
        part = pl.ds(pl.multiple_of(to_kv * kv_cols, 128), kv_cols)
        partial_sum = dot32(hidden2, down2_v[:, part]).astype(BF16)
        for t in range(n_tp):
            sum2_send[i, t] = partial_sum[:, t * cols : (t + 1) * cols]
        for j, to_tp in enumerate(all_tp):
            if i < n_kv - 1 or j:
                send(
                    sum2_send.at[i, to_tp], sum2_all.at[me], SUM2, i * n_tp + j, me, to_kv, to_tp
                )
    sum2_all[me] = sum2_send[n_kv - 1, tp]
    own = after_of(kv)
    mine = own[:, :cols]
    for t in range(1, n_tp):
        mine = jnp.where(tp == t, own[:, t * cols : (t + 1) * cols], mine)
    for k, t in far_peers:
        arrive(sum2_all.at[k * n_tp + t], SUM2, k * n_tp + t)
    summed = sum2_all[0].astype(F32)
    for i in range(1, n):
        summed = summed + sum2_all[i].astype(F32)
    result_v[...] = (mine + 0.5 * summed).astype(BF16)
    out_copies.append(load(result_v, result))
    for copy in sends:
        copy.wait_send()
    for copy in out_copies:
        copy.wait()


def finish_kernel(
    result,
    step_x,
    retain,
    keys_b,
    new_x,
    new_bc,
    state,
    result_out,
    state_out,
    new_x_out,
    new_bc_out,
    result_v,
    step_x_v,
    retain_v,
    b_v,
    new_x_v,
    new_bc_v,
    old,
    fresh,
    in_sem,
    out_sem,
    old_sem,
    fresh_sem,
):
    seqs, inner, state_size = state.shape
    groups = keys_b.shape[1] // state_size
    span = inner // groups

    def start(source, target, sem):
        copy = pltpu.make_async_copy(source, target, sem)
        copy.start()
        return copy

    needed = [
        start(step_x, step_x_v, in_sem.at[0]),
        start(retain, retain_v, in_sem.at[1]),
        start(keys_b, b_v, in_sem.at[2]),
    ]
    blocks = [
        (s, g, pl.ds(g * span, span)) for g in range(groups) for s in range(seqs)
    ]
    reads = [start(state.at[s, part], old.at[s, part], old_sem.at[s, g]) for s, g, part in blocks]
    passed = [
        (start(source, held, in_sem.at[3 + i]), held, target)
        for i, (source, held, target) in enumerate(
            (
                (result, result_v, result_out),
                (new_x, new_x_v, new_x_out),
                (new_bc, new_bc_v, new_bc_out),
            )
        )
    ]
    for copy in needed:
        copy.wait()
    rows = jnp.concatenate([retain_v[...], step_x_v[...]] * (8 // (2 * seqs)), axis=0)
    columns = rows.T
    writes = []
    for read, (s, g, part) in zip(reads, blocks):
        read.wait()
        here = slice(g * span, (g + 1) * span)
        fresh[s, part, :] = (
            columns[here, s : s + 1] * old[s, part, :]
            + columns[here, seqs + s : seqs + s + 1]
            * b_v[s : s + 1, g * state_size : (g + 1) * state_size]
        )
        writes.append(start(fresh.at[s, part], state_out.at[s, part], fresh_sem.at[s, g]))
    for i, (copy, held, target) in enumerate(passed):
        copy.wait()
        writes.append(start(held, target, out_sem.at[i]))
    for copy in writes:
        copy.wait()


def per_device(n_kv, n_tp, *args):
    (
        tokens,
        mlp1_gain,
        mlp1_gate,
        mlp1_up,
        mlp1_down,
        mixer_gain,
        proj_z,
        proj_x,
        proj_bc,
        proj_dt,
        conv_x,
        conv_bc,
        window_x,
        window_bc,
        ssm_state,
        dt_bias,
        log_rate,
        skip_gain,
        group_gain,
        out_weight,
        mlp2_gain,
        mlp2_gate,
        mlp2_up,
        mlp2_down,
    ) = args
    rows, cols = tokens.shape
    if cols % 128 or n_kv * n_tp > 16 or rows % 8 or 8 % (2 * window_x.shape[0]):
        return plain_device(*args)
    n = n_kv * n_tp
    kv_cols = cols * n_tp
    seqs, heads = window_x.shape[0], proj_dt.shape[1]
    inner, group_width = proj_z.shape[1], proj_bc.shape[2]
    state_size = ssm_state.shape[3]
    groups = group_width // state_size
    taps = conv_x.shape[0]
    operands = (
        tokens,
        mlp1_gain[None],
        mlp1_gate.T,
        mlp1_up.T,
        mlp1_down,
        mixer_gain[None],
        proj_z,
        proj_x,
        proj_bc,
        proj_dt.T,
        conv_x,
        conv_bc,
        jnp.swapaxes(window_x, 0, 1),
        window_bc,
        ssm_state.reshape(seqs, inner, state_size),
        dt_bias[None],
        log_rate[None],
        skip_gain[None],
        group_gain[None],
        out_weight,
        mlp2_gain[None],
        mlp2_gate.T,
        mlp2_up.T,
        mlp2_down,
    )
    vmem = [pltpu.VMEM(a.shape, a.dtype) for a in operands]
    scratch = vmem + [
        pltpu.VMEM((seqs, inner, state_size), BF16),
        pltpu.VMEM((2, proj_bc.shape[0], group_width), BF16),
        pltpu.VMEM((n, rows, cols), BF16),
        pltpu.VMEM((n_kv, rows, kv_cols), BF16),
        pltpu.VMEM((n, rows, kv_cols), BF16),
        pltpu.VMEM((n_kv, seqs, 2 * inner + 2 * group_width), BF16),
        pltpu.VMEM((n_kv, seqs, 2 * inner + 2 * group_width), BF16),
        pltpu.VMEM((n_kv, seqs, 128), F32),
        pltpu.VMEM((n_kv, seqs, 128), F32),
        pltpu.VMEM((n_kv, rows, kv_cols), BF16),
        pltpu.VMEM((n_kv, seqs, inner), BF16),
        pltpu.VMEM((n, rows, kv_cols), BF16),
        pltpu.VMEM((n_kv, n_tp, rows, cols), BF16),
        pltpu.VMEM((n, rows, cols), BF16),
    ]
    shapes = (
        jax.ShapeDtypeStruct((rows, cols), BF16),
        jax.ShapeDtypeStruct((seqs, inner), F32),
        jax.ShapeDtypeStruct((seqs, inner), F32),
        jax.ShapeDtypeStruct((seqs, group_width), F32),
        jax.ShapeDtypeStruct((taps - 1, seqs, inner), BF16),
        jax.ShapeDtypeStruct(window_bc.shape, BF16),
    )
    scratch += [pltpu.VMEM(a.shape, a.dtype) for a in shapes]
    scratch += [
        pltpu.SemaphoreType.DMA((2 * n + 40,)),
        pltpu.SemaphoreType.DMA((PHASES, n)),
        pltpu.SemaphoreType.DMA((PHASES, n)),
    ]
    anywhere = pl.BlockSpec(memory_space=pl.ANY)
    small, state_flat = shapes, operands[14]
    result, step_x, retain, keys_b, new_x, new_bc = pl.pallas_call(
        functools.partial(fused_kernel, n_kv, n_tp),
        out_shape=shapes,
        in_specs=[anywhere] * len(operands),
        out_specs=[anywhere] * len(shapes),
        scratch_shapes=scratch,
        compiler_params=pltpu.CompilerParams(
            collective_id=0, has_side_effects=True, vmem_limit_bytes=60 * 1024 * 1024
        ),
    )(*operands)
    result, new_state, new_x, new_bc = pl.pallas_call(
        finish_kernel,
        out_shape=(
            shapes[0],
            jax.ShapeDtypeStruct(state_flat.shape, F32),
            shapes[4],
            shapes[5],
        ),
        in_specs=[anywhere] * 7,
        out_specs=[anywhere] * 4,
        scratch_shapes=[pltpu.VMEM(a.shape, a.dtype) for a in small]
        + [
            pltpu.VMEM(state_flat.shape, F32),
            pltpu.VMEM(state_flat.shape, F32),
            pltpu.SemaphoreType.DMA((6,)),
            pltpu.SemaphoreType.DMA((3,)),
            pltpu.SemaphoreType.DMA((seqs, groups)),
            pltpu.SemaphoreType.DMA((seqs, groups)),
        ],
    )(result, step_x, retain, keys_b, new_x, new_bc, state_flat)
    return (result, new_state.reshape(ssm_state.shape), jnp.swapaxes(new_x, 0, 1), new_bc)


def solution(mesh):
    placed = (
        P("dp", ("kv", "tp")),
        P(),
        P(None, ("kv", "tp")),
        P(None, ("kv", "tp")),
        P(("kv", "tp"), None),
        P(),
        P("kv", "tp"),
        P("kv", "tp"),
        P("kv", None, "tp"),
        P("kv", "tp"),
        P(None, "tp"),
        P(None, None, "tp"),
        P(("dp", "kv"), None, "tp"),
        P(("dp", "kv"), None, None, "tp"),
        P(("dp", "kv"), "tp", None, None),
        P("tp"),
        P("tp"),
        P("tp"),
        P("tp"),
        P("tp", "kv"),
        P(),
        P(None, ("kv", "tp")),
        P(None, ("kv", "tp")),
        P(("kv", "tp"), None),
    )
    return jax.shard_map(
        functools.partial(per_device, mesh.shape["kv"], mesh.shape["tp"]),
        mesh=mesh,
        in_specs=placed,
        out_specs=(
            P("dp", ("kv", "tp")),
            P(("dp", "kv"), "tp", None, None),
            P(("dp", "kv"), None, "tp"),
            P(("dp", "kv"), None, None, "tp"),
        ),
        check_vma=False,
    )
```
